512 devices in a mesh: gr: 2 (over z_hi), fs: 32 (over z_lo, y), tp: 8 (over x, core).
Axes of the slice: x: 4, y: 8, z: 8 (z_hi: 2, z_lo: 4; z = z_hi * 4 + z_lo), core: 2. Of those that a mesh axis runs over, the one named last changes fastest.
Arguments:
- prompt: bfloat16 [16, 256, 2048], P(('gr', 'tp')), as said below
- norm_gain: float32 [2, 2048], P(None, 'fs'), may hold values from 0.1 to 1.9
- gate_weight: float32 [2, 2048, 4096], P(None, 'fs', ('gr', 'tp')), may hold values from -0.125 to 0.125
- up_weight: float32 [2, 2048, 4096], P(None, 'fs', ('gr', 'tp')), may hold values from -0.125 to 0.125
- down_weight: float32 [2, 4096, 2048], P(None, 'fs', ('gr', 'tp')), may hold values from -0.09375 to 0.09375
Outputs:
- gate_sampler: bfloat16 [2, 2048, 4096], P(None, None, 'fs')
- up_sampler: bfloat16 [2, 2048, 4096], P(None, None, 'fs')
- down_sampler: bfloat16 [2, 4096, 2048], P(None, 'fs')
- mixed: bfloat16 [16, 256, 2048], P(('gr', 'tp'))
The draws below stay inside these ranges and needn't reach their ends.
Inputs may be any that keep to these rules, and one draw needn't show every extreme that they name: prompt features have scales that differ from feature to feature.
All inputs are finite; a program needn't handle non-finite values.
Results may differ from the reference program's by a relative error of at most 0.0043.
Values may be sent and summed in bfloat16 or wider, within the bound.
No kernel may reach another device: no remote copies, remote signals or barrier semaphores. Data moves between devices by JAX's collectives and lax.ppermute only.
A program may use at most 64 MiB of HBM per device.

```python
import jax
import jax.numpy as jnp
from jax import lax

D = 2048
FF = 4096
ROWS = 256
REQS = 16


def draw_prompt(key, part):
    first = jax.random.fold_in(jax.random.fold_in(key, 7), 0)
    column = jnp.arange(D, dtype=jnp.float32) / (D - 1.0)
    values = jax.random.normal(first, (REQS, ROWS, D), jnp.float32)
    scales = jnp.exp(column * 1.1)
    values = values * scales[None, None, :] * 0.6
    return jnp.clip(values, -6.0, 6.0).astype(jnp.bfloat16)


def level_of(key, extent, pieces, smallest, high):
    loudness, own = 1.0, jax.random.fold_in(key, 6)
    for dim, shards_of in pieces:
        steps = jnp.exp(jax.random.uniform(jax.random.fold_in(own, dim), (shards_of,), jnp.float32, smallest / len(pieces), high / len(pieces)))
        loudness = loudness * jnp.repeat(steps, extent[dim] // shards_of).reshape([-1 if axis == dim else 1 for axis in range(len(extent))])
    return loudness


def centred(rng, extent, scale, most, pieces=(), held_as=jnp.bfloat16):
    entries = jax.random.normal(rng, extent, jnp.float32) * scale
    if len(pieces) > 0:
        entries = level_of(rng, extent, pieces, -0.22, 0.18) * entries
    return jnp.clip(entries, min=-most, max=most).astype(held_as)


def setup_inputs(seed: int = 0) -> dict:
    splits = jax.random.split(jax.random.key(seed), 6)
    prompt = draw_prompt(jax.random.fold_in(splits[5], 71), 0)
    norm_gain = jnp.clip(1.0 + 0.18 * jax.random.normal(splits[1], (2, D), jnp.float32), 0.1, 1.9)
    gate_weight = centred(splits[2], (2, D, FF), D ** -0.5, 0.125, ((1, 32), (2, 16)), jnp.float32)
    up_weight = centred(splits[3], (2, D, FF), D ** -0.5, 0.125, ((1, 32), (2, 16)), jnp.float32)
    down_weight = centred(splits[4], (2, FF, D), FF ** -0.5, 0.09375, ((1, 32), (2, 16)), jnp.float32)
    return {"prompt": prompt, "norm_gain": norm_gain, "gate_weight": gate_weight, "up_weight": up_weight, "down_weight": down_weight}


norm_eps = 1e-06

def reference(prompt, norm_gain, gate_weight, up_weight, down_weight):
    gates = (norm_gain[:, :, None] * gate_weight).astype(jnp.bfloat16)
    ups = (norm_gain[:, :, None] * up_weight).astype(jnp.bfloat16)
    downs = down_weight.astype(jnp.bfloat16)
    total_rows = prompt.shape[0] * prompt.shape[1]
    stream = prompt.astype(jnp.float32).reshape(total_rows, D)
    for half_step in range(2):
        normed = (stream * lax.rsqrt(lax.optimization_barrier(jnp.mean(stream * stream, axis=-1, keepdims=True)) + norm_eps)).astype(jnp.bfloat16)
        gate_act = jnp.dot(normed, gates[half_step], preferred_element_type=jnp.float32)
        up_act = jnp.dot(normed, ups[half_step], preferred_element_type=jnp.float32)
        hidden = (jax.nn.silu(gate_act) * up_act).astype(jnp.bfloat16)
        projected = jnp.dot(hidden, downs[half_step], preferred_element_type=jnp.float32)
        stream = stream + 0.5 * projected
    mixed = stream.astype(jnp.bfloat16).reshape(prompt.shape)
    return (gates, ups, downs, mixed)
```

```python
import jax
import jax.numpy as jnp
from jax import lax
from jax.sharding import Mesh
from jax.sharding import PartitionSpec as P

norm_eps = 1e-06
bf16 = jnp.bfloat16
f32 = jnp.float32

AXES = ("gr", "zl", "yh", "yl", "x", "core")
SIZES = (2, 4, 4, 2, 4, 2)
FS = ("zl", "yh", "yl")
GT = ("gr", "x", "core")


def device(gr, fs, tp):
    return gr * 256 + fs * 8 + tp


def weight_moves(k):
    moves = []
    for gr in range(2):
        for fs in range(32):
            for tp in range(8):
                s = (fs >> 1) & 1
                to = device(s ^ k, 2 * (8 * gr + tp) + (fs & 1), fs >> 2)
                moves.append((device(gr, fs, tp), to))
    return moves


def down_moves(k):
    moves = []
    for gr in range(2):
        for fs in range(32):
            for tp in range(8):
                b = fs & 1
                moves.append((device(gr, fs, tp), device(b ^ k, (fs & ~1) + gr, tp)))
    return moves


def in_order(first, second, swapped):
    return jnp.where(swapped, second, first), jnp.where(swapped, first, second)


def to_everyone(value, axes, count):
    return lax.all_to_all(
        jnp.broadcast_to(value[None], (count, *value.shape)), axes, 0, 0, tiled=True
    )


def weights_for_sampling(norm_gain, gate_weight, up_weight, down_weight):
    gain = norm_gain[:, :, None]
    gate = (gain * gate_weight).astype(bf16)
    up = (gain * up_weight).astype(bf16)
    block = jnp.stack([gate, up]).reshape(256, 256)
    down = down_weight.astype(bf16).reshape(256, 128)
    swapped = lax.axis_index("gr") == 1
    got = [lax.ppermute(block, AXES, weight_moves(k)) for k in range(2)]
    rows = in_order(*got, swapped)
    got = [lax.ppermute(down, AXES, down_moves(k)) for k in range(2)]
    down_rows = in_order(*got, swapped)
    halves = []
    for b in range(2):
        cols = slice(128 * b, 128 * b + 128)
        halves.append(jnp.concatenate([rows[0][:, cols], rows[1][:, cols], down_rows[b]], axis=0))
    sends = jnp.broadcast_to(jnp.stack(halves)[:, None], (2, 4, 768, 128)).reshape(8, 768, 128)
    got = lax.all_to_all(sends, ("yl", "x"), 0, 0, tiled=True)
    got = to_everyone(got, "core", 2)
    got = got.reshape(2, 2, 4, 768, 128)
    gu = got[:, :, :, :512].reshape(2, 2, 4, 2, 2, 2, 64, 128)
    gu = gu.transpose(4, 5, 2, 0, 3, 1, 6, 7).reshape(2, 2, 2048, 128)
    dn = got[:, :, :, 512:].reshape(2, 2, 4, 2, 128, 128)
    dn = dn.transpose(3, 4, 1, 2, 0, 5).reshape(2, 128, 2048)
    return gu[0], gu[1], dn


def normalised(stream):
    return (
        stream * lax.rsqrt(jnp.mean(stream * stream, axis=-1, keepdims=True) + norm_eps)
    ).astype(bf16)


def per_device(prompt, norm_gain, gate_weight, up_weight, down_weight):
    gates, ups, downs = weights_for_sampling(norm_gain, gate_weight, up_weight, down_weight)
    tokens, width = prompt.shape[1:]
    normed = normalised(prompt[0].astype(f32))
    count = tokens // 32
    mine = lax.dynamic_slice_in_dim(prompt[0], lax.axis_index(FS) * count, count, 0).astype(f32)
    for k in range(2):
        gate_act = jnp.dot(normed, gates[k], preferred_element_type=f32)
        up_act = jnp.dot(normed, ups[k], preferred_element_type=f32)
        hidden = (jax.nn.silu(gate_act) * up_act).astype(bf16)
        part = jnp.dot(hidden, downs[k], preferred_element_type=f32).astype(bf16)
        parts = lax.all_to_all(part.reshape(32, count, width), FS, 0, 0, tiled=True)
        mine = mine + 0.5 * jnp.sum(parts.astype(f32), axis=0)
        sent = normalised(mine) if k == 0 else mine.astype(bf16)
        normed = to_everyone(sent, FS, 32).reshape(tokens, width)
    return gates, ups, downs, normed[None]


def solution(mesh):
    fine = Mesh(mesh.devices.reshape(SIZES), AXES)
    in_specs = (P(GT, None, None), P(None, FS), P(None, FS, GT), P(None, FS, GT), P(None, FS, GT))
    out_specs = (P(None, None, FS), P(None, None, FS), P(None, FS, None), P(GT, None, None))
    return jax.shard_map(
        per_device, mesh=fine, in_specs=in_specs, out_specs=out_specs, check_vma=False
    )
```

```python
import jax
import jax.numpy as jnp
from jax import lax
from jax.experimental import pallas as pl
from jax.experimental.pallas import tpu as pltpu
from jax.sharding import Mesh
from jax.sharding import PartitionSpec as P

norm_eps = 1e-06
bf16 = jnp.bfloat16
f32 = jnp.float32

AXES = ("gr", "zl", "yh", "yl", "x", "core")
SIZES = (2, 4, 4, 2, 4, 2)
FS = ("zl", "yh", "yl")
GT = ("gr", "x", "core")


def device(gr, fs, tp):
    return gr * 256 + fs * 8 + tp


def everyone():
    return [(gr, fs, tp) for gr in range(2) for fs in range(32) for tp in range(8)]


def weight_moves(k):
    moves = []
    for gr, fs, tp in everyone():
        to = device(((fs >> 1) & 1) ^ k, 2 * (8 * gr + tp) + (fs & 1), fs >> 2)
        moves.append((device(gr, fs, tp), to))
    return moves


def down_moves(k):
    moves = []
    for gr, fs, tp in everyone():
        zl, y = fs >> 3, fs & 7
        to_fs = (2 * gr + (tp >> 2)) * 8 + (y & 6) + (zl & 1)
        to_tp = ((tp >> 1) & 1) * 4 + (zl >> 1) * 2 + (tp & 1)
        moves.append((device(gr, fs, tp), device((y & 1) ^ k, to_fs, to_tp)))
    return moves


def in_order(first, second, swapped):
    return jnp.where(swapped, second, first), jnp.where(swapped, first, second)


def to_everyone(value, axes, count):
    return lax.all_to_all(
        jnp.broadcast_to(value[None], (count, *value.shape)), axes, 0, 0, tiled=True
    )


def weights(norm_gain, gate_weight, up_weight, down_weight):
    gain = norm_gain[:, :, None]
    gate = (gain * gate_weight).astype(bf16)
    up = (gain * up_weight).astype(bf16)
    block = jnp.concatenate([gate[0], up[0], gate[1], up[1]], axis=0)
    down = down_weight.astype(bf16).reshape(256, 128)
    served = lax.all_gather(down, GT, axis=0, tiled=True)
    served = served.reshape(16, 2, 128, 128).transpose(1, 2, 0, 3).reshape(2, 128, 2048)
    high = lax.axis_index("gr") == 1
    got = [lax.ppermute(block, AXES, weight_moves(k)) for k in range(2)]
    rows = in_order(*got, high)
    got = [lax.ppermute(down, AXES, down_moves(k)) for k in range(2)]
    down_rows = in_order(*got, high)
    first = []
    for b in range(2):
        cols = slice(128 * b, 128 * b + 128)
        first.append(
            jnp.concatenate([rows[0][:128, cols], rows[1][:128, cols], down_rows[b]], axis=0)
        )
    sends = []
    for x in range(4):
        for b in range(2):
            cols = slice(128 * b, 128 * b + 128)
            quarter = [
                rows[s][at + 16 * x : at + 16 * x + 16, cols] for s in range(2) for at in (128, 192)
            ]
            sends.append(jnp.concatenate([first[b], *quarter], axis=0))
    got = lax.all_to_all(jnp.stack(sends), ("x", "yl"), 0, 0, tiled=True)
    late = lax.all_gather(got[:, 512:].reshape(512, 128), ("x", "core"), axis=0, tiled=True)
    early = to_everyone(got[:, :512], "core", 2).reshape(2, 4, 2, 512, 128)
    return early, late.reshape(8, 512, 128), served


def gathered_early(got, both):
    for x in range(4):
        for core in range(2):
            for s in range(2):
                for b in range(2):
                    at = 64 * (8 * x + 4 * core + 2 * s + b)
                    both[at : at + 64, :128] = got[core, x, b, 128 * s : 128 * s + 64]
                    both[at : at + 64, 128:] = got[core, x, b, 128 * s + 64 : 128 * s + 128]


def gathered_late(got, both):
    for to in range(4):
        for core in range(2):
            for x in range(4):
                for b in range(2):
                    for s in range(2):
                        at = 64 * (8 * x + 4 * core + 2 * s + b) + 16 * to
                        come = 64 * (2 * x + b) + 32 * s
                        line = got[2 * to + core, come : come + 32]
                        both[at : at + 16, :128] = line[:16]
                        both[at : at + 16, 128:] = line[16:]


def up_body(late, stream, got, gate, up, hidden, both):
    (gathered_late if late else gathered_early)(got, both)
    gate[...] = both[:, :128]
    up[...] = both[:, 128:]
    squares = jnp.zeros((256, 1), f32)
    for z in range(4):
        part = (stream[z] if late else stream[:, 512 * z : 512 * z + 512]).astype(f32)
        squares = squares + jnp.sum(part * part, axis=1, keepdims=True)
    scale = lax.rsqrt(squares * (1.0 / 2048) + norm_eps)
    act = jnp.zeros((256, 256), f32)
    for z in range(4):
        part = (stream[z] if late else stream[:, 512 * z : 512 * z + 512]).astype(f32)
        normed = (part * scale).astype(bf16)
        act = act + jnp.dot(normed, both[512 * z : 512 * z + 512], preferred_element_type=f32)
    gate_act, up_act = act[:, :128], act[:, 128:]
    hidden[...] = (gate_act / (1.0 + jnp.exp(-gate_act)) * up_act).astype(bf16)


def up_call(late, stream, got):
    def body(*refs):
        up_body(late, *refs)

    return pl.pallas_call(
        body,
        out_shape=(
            jax.ShapeDtypeStruct((2048, 128), bf16),
            jax.ShapeDtypeStruct((2048, 128), bf16),
            jax.ShapeDtypeStruct((256, 128), bf16),
        ),
        scratch_shapes=[pltpu.VMEM((2048, 256), bf16)],
        name="late_up" if late else "early_up",
    )(stream, got)


def down_call(layer, hidden, got):
    def body(hidden, got, out, units, square):
        for z in range(4):
            units[:, 128 * z : 128 * z + 128] = hidden[z]
            for n in range(4):
                square[128 * z : 128 * z + 128, 128 * n : 128 * n + 128] = got[
                    n & 1, (n & 2) + (z >> 1), z & 1, 256 + 128 * layer : 384 + 128 * layer
                ]
        out[...] = jnp.dot(units[...], square[...], preferred_element_type=f32).astype(bf16)

    return pl.pallas_call(
        body,
        out_shape=jax.ShapeDtypeStruct((256, 512), bf16),
        scratch_shapes=[pltpu.VMEM((256, 512), bf16), pltpu.VMEM((512, 512), bf16)],
        name="down",
    )(hidden, got)


def per_device(prompt, norm_gain, gate_weight, up_weight, down_weight):
    early, late, served = weights(norm_gain, gate_weight, up_weight, down_weight)
    stream = prompt[0]
    mine = lax.dynamic_slice(
        stream, (lax.axis_index(("yh", "yl")) * 32, lax.axis_index("zl") * 512), (32, 512)
    ).astype(f32)
    gates, ups = [], []
    for layer in range(2):
        gate, up, hidden = up_call(layer == 1, stream, late if layer else early)
        gates.append(gate)
        ups.append(up)
        part = down_call(layer, to_everyone(hidden, "zl", 4), early)
        parts = lax.all_to_all(part.reshape(8, 32, 512), ("yh", "yl"), 0, 0, tiled=True)
        mine = mine + 0.5 * jnp.sum(parts.astype(f32), axis=0)
        stream = to_everyone(mine.astype(bf16), FS, 32).reshape(4, 256, 512)
    mixed = jnp.concatenate(list(stream), axis=1)
    return jnp.stack(gates), jnp.stack(ups), served, mixed[None]


def solution(mesh):
    fine = Mesh(mesh.devices.reshape(SIZES), AXES)
    in_specs = (P(GT, None, None), P(None, FS), P(None, FS, GT), P(None, FS, GT), P(None, FS, GT))
    out_specs = (P(None, None, FS), P(None, None, FS), P(None, FS, None), P(GT, None, None))
    return jax.shard_map(
        per_device, mesh=fine, in_specs=in_specs, out_specs=out_specs, check_vma=False
    )
```

```python
import jax
import jax.numpy as jnp
from jax import lax
from jax.experimental import pallas as pl
from jax.experimental.pallas import tpu as pltpu
from jax.sharding import Mesh
from jax.sharding import PartitionSpec as P

norm_eps = 1e-06
bf16 = jnp.bfloat16
f32 = jnp.float32

AXES = ("gr", "zl", "yh", "yl", "x", "core")
SIZES = (2, 4, 4, 2, 4, 2)
FS = ("zl", "yh", "yl")
GT = ("gr", "x", "core")
SWAP = [(0, 1), (1, 0)]


def device(gr, fs, tp):
    return gr * 256 + fs * 8 + tp


def everyone():
    return [(gr, fs, tp) for gr in range(2) for fs in range(32) for tp in range(8)]


def weight_moves(k):
    moves = []
    for gr, fs, tp in everyone():
        to = device(((fs >> 1) & 1) ^ k, 2 * (8 * gr + tp) + (fs & 1), fs >> 2)
        moves.append((device(gr, fs, tp), to))
    return moves


def in_order(first, second, swapped):
    return jnp.where(swapped, second, first), jnp.where(swapped, first, second)


def halves_to_all(blocks):
    rows = blocks[0].shape[0]
    sends = jnp.broadcast_to(jnp.stack(blocks)[None], (4, 2, rows, 128)).reshape(8, rows, 128)
    return lax.all_to_all(sends, ("x", "yl"), 0, 0, tiled=True)


def columns(rows, b):
    return [r[:, 128 * b : 128 * b + 128] for r in rows]


def gather_rows(core, own, other, both):
    mine = core == 0
    for x in range(4):
        for b in range(2):
            for s in range(2):
                mn = own[2 * x + b, 128 * s : 128 * s + 128]
                ot = other[2 * x + b, 128 * s : 128 * s + 128]
                for c in range(2):
                    line = jnp.where(mine, mn, ot) if c == 0 else jnp.where(mine, ot, mn)
                    at = 64 * (8 * x + 4 * c + 2 * s + b)
                    both[at : at + 64, :128] = line[:64]
                    both[at : at + 64, 128:] = line[64:]


def up_call(late, stream, own, other):
    def part_of(stream, z):
        if late:
            return stream[z // 2, :, 512 * (z % 2) : 512 * (z % 2) + 512].astype(f32)
        return stream[:, 512 * z : 512 * z + 512].astype(f32)

    def body(stream, own, other, gate, up, hidden, both):
        gather_rows(lax.axis_index("core"), own, other, both)
        gate[...] = both[:, :128]
        up[...] = both[:, 128:]
        squares = jnp.zeros((256, 1), f32)
        for z in range(4):
            part = part_of(stream, z)
            squares = squares + jnp.sum(part * part, axis=1, keepdims=True)
        scale = lax.rsqrt(squares * (1.0 / 2048) + norm_eps)
        act = jnp.zeros((256, 256), f32)
        for z in range(4):
            normed = (part_of(stream, z) * scale).astype(bf16)
            act = act + jnp.dot(normed, both[512 * z : 512 * z + 512], preferred_element_type=f32)
        gate_act, up_act = act[:, :128], act[:, 128:]
        hidden[...] = (gate_act / (1.0 + jnp.exp(-gate_act)) * up_act).astype(bf16)

    return pl.pallas_call(
        body,
        out_shape=(
            jax.ShapeDtypeStruct((2048, 128), bf16),
            jax.ShapeDtypeStruct((2048, 128), bf16),
            jax.ShapeDtypeStruct((256, 128), bf16),
        ),
        scratch_shapes=[pltpu.VMEM((2048, 256), bf16)],
        name="late_up" if late else "early_up",
    )(stream, own, other)


def down_rows_call(own, other):
    def body(own, other, keep, send):
        mine = lax.axis_index("core") == 0
        even = lax.axis_index("yl") == 0
        for x in range(4):
            for k in range(2):
                at = 256 + 128 * k
                mn = [own[2 * x + b, at : at + 128] for b in range(2)]
                ot = [other[2 * x + b, at : at + 128] for b in range(2)]
                for c in range(2):
                    a, b = (mn, ot) if c == 0 else (ot, mn)
                    line = [jnp.where(mine, a[i], b[i]) for i in range(2)]
                    col = 256 * x + 128 * c
                    keep[k, :, col : col + 128] = jnp.where(even, line[0], line[1])
                    send[k, :, col : col + 128] = jnp.where(even, line[1], line[0])

    shape = jax.ShapeDtypeStruct((2, 128, 1024), bf16)
    return pl.pallas_call(body, out_shape=(shape, shape), name="down_rows")(own, other)


def down_call(layer, own, other, keep, send):
    def body(own, other, keep, send, out):
        act = jnp.dot(own[...], keep[layer], preferred_element_type=f32)
        act = act + jnp.dot(other[...], send[layer], preferred_element_type=f32)
        out[...] = act.astype(bf16)

    return pl.pallas_call(
        body, out_shape=jax.ShapeDtypeStruct((256, 1024), bf16), name="down"
    )(own, other, keep, send)


def per_device(prompt, norm_gain, gate_weight, up_weight, down_weight):
    gain = norm_gain[:, :, None]
    gate = (gain * gate_weight).astype(bf16)
    up = (gain * up_weight).astype(bf16)
    high = lax.axis_index("gr") == 1
    rows = []
    for layer in range(2):
        block = jnp.concatenate([gate[layer], up[layer]], axis=0)
        got = [lax.ppermute(block, AXES, weight_moves(k)) for k in range(2)]
        rows.append(in_order(*got, high))
    down = down_weight.astype(bf16).reshape(256, 128)
    downs = in_order(down, lax.ppermute(down, "gr", SWAP), high)
    early = halves_to_all([jnp.concatenate([*columns(rows[0], b), downs[b]]) for b in range(2)])
    early = early, lax.ppermute(early, "core", SWAP)
    late = halves_to_all([jnp.concatenate(columns(rows[1], b)) for b in range(2)])
    late = late, lax.ppermute(late, "core", SWAP)
    keep, send = down_rows_call(*early)
    came = lax.ppermute(send, "yl", SWAP)

    stream = prompt[0]
    yl = lax.axis_index("yl")
    mine = lax.dynamic_slice(
        stream, (lax.axis_index(("zl", "yh")) * 16, yl * 1024), (16, 1024)
    ).astype(f32)
    gates, ups = [], []
    for layer in range(2):
        gate, up, hidden = up_call(layer == 1, stream, *(late if layer else early))
        gates.append(gate)
        ups.append(up)
        part = down_call(layer, hidden, lax.ppermute(hidden, "yl", SWAP), keep, send)
        parts = lax.all_to_all(part.reshape(16, 16, 1024), ("zl", "yh"), 0, 0, tiled=True)
        mine = mine + 0.5 * jnp.sum(parts.astype(f32), axis=0)
        sends = jnp.broadcast_to(mine.astype(bf16)[None], (32, 16, 1024))
        stream = lax.all_to_all(sends, ("yl", "zl", "yh"), 0, 0, tiled=True).reshape(2, 256, 1024)
    mixed = jnp.concatenate(list(stream), axis=1)
    served = jnp.concatenate(in_order(keep, came, yl == 1), axis=2)
    return jnp.stack(gates), jnp.stack(ups), served, mixed[None]


def solution(mesh):
    fine = Mesh(mesh.devices.reshape(SIZES), AXES)
    in_specs = (P(GT, None, None), P(None, FS), P(None, FS, GT), P(None, FS, GT), P(None, FS, GT))
    out_specs = (P(None, None, FS), P(None, None, FS), P(None, FS, None), P(GT, None, None))
    return jax.shard_map(
        per_device, mesh=fine, in_specs=in_specs, out_specs=out_specs, check_vma=False
    )
```

```python
import jax
import jax.numpy as jnp
from jax import lax
from jax.experimental import pallas as pl
from jax.experimental.pallas import tpu as pltpu
from jax.sharding import Mesh
from jax.sharding import PartitionSpec as P


norm_eps = 1e-06
bf16 = jnp.bfloat16
f32 = jnp.float32

AXES = ("gr", "zl", "yh", "yl", "x", "core")
SIZES = (2, 4, 4, 2, 4, 2)
FS = ("zl", "yh", "yl")
GT = ("gr", "x", "core")
SWAP = [(0, 1), (1, 0)]


def device(gr, fs, tp):
    return gr * 256 + fs * 8 + tp


def everyone():
    return [(gr, fs, tp) for gr in range(2) for fs in range(32) for tp in range(8)]


def weight_moves(k):
    moves = []
    for gr, fs, tp in everyone():
        to = device(((fs >> 1) & 1) ^ k, 2 * (8 * gr + tp) + (fs & 1), fs >> 2)
        moves.append((device(gr, fs, tp), to))
    return moves


def in_vmem(value):
    return pltpu.with_memory_space_constraint(value, pltpu.VMEM)


def kernel(body, outs, scratch=()):
    here = pl.BlockSpec(memory_space=pltpu.VMEM)

    def call(*args):
        return pl.pallas_call(
            body,
            in_specs=[here] * len(args),
            out_specs=tuple(here for _ in outs),
            out_shape=tuple(pltpu.VMEM(shape, bf16) for shape in outs),
            scratch_shapes=[pltpu.VMEM(shape, bf16) for shape in scratch],
            compiler_params=pltpu.CompilerParams(vmem_limit_bytes=16 << 20),
        )(*[in_vmem(a) for a in args])

    return call


def in_order(first, second, swapped):
    return jnp.where(swapped, second, first), jnp.where(swapped, first, second)


def halves_to_all(blocks):
    rows = blocks[0].shape[0]
    sends = jnp.broadcast_to(jnp.stack(blocks)[None], (4, 2, rows, 128)).reshape(8, rows, 128)
    return lax.all_to_all(sends, ("x", "yl"), 0, 0, tiled=True)


def columns(rows, b):
    return [r[:, 128 * b : 128 * b + 128] for r in rows]


def gather_rows(core, own, other, both):
    mine = core == 0
    for x in range(4):
        for b in range(2):
            for s in range(2):
                mn = own[2 * x + b, 128 * s : 128 * s + 128]
                ot = other[2 * x + b, 128 * s : 128 * s + 128]
                for c in range(2):
                    line = jnp.where(mine, mn, ot) if c == 0 else jnp.where(mine, ot, mn)
                    at = 64 * (8 * x + 4 * c + 2 * s + b)
                    both[at : at + 64, :128] = line[:64]
                    both[at : at + 64, 128:] = line[64:]


def up_call(late, stream, own, other):
    def part_of(stream, z):
        if late:
            return stream[z // 2, :, 512 * (z % 2) : 512 * (z % 2) + 512].astype(f32)
        return stream[:, 512 * z : 512 * z + 512].astype(f32)

    def body(stream, own, other, gate, up, hidden, both):
        gather_rows(lax.axis_index("core"), own, other, both)
        gate[...] = both[:, :128]
        up[...] = both[:, 128:]
        squares = jnp.zeros((256, 1), f32)
        for z in range(4):
            part = part_of(stream, z)
            squares = squares + jnp.sum(part * part, axis=1, keepdims=True)
        scale = lax.rsqrt(squares * (1.0 / 2048) + norm_eps)
        act = jnp.zeros((256, 256), f32)
        for z in range(4):
            normed = (part_of(stream, z) * scale).astype(bf16)
            act = act + jnp.dot(normed, both[512 * z : 512 * z + 512], preferred_element_type=f32)
        gate_act, up_act = act[:, :128], act[:, 128:]
        hidden[...] = (gate_act / (1.0 + jnp.exp(-gate_act)) * up_act).astype(bf16)

    outs = ((2048, 128), (2048, 128), (256, 128))
    return kernel(body, outs, ((2048, 256),))(stream, own, other)


def down_rows_call(own, other):
    def body(own, other, keep, send):
        mine = lax.axis_index("core") == 0
        even = lax.axis_index("yl") == 0
        for x in range(4):
            for k in range(2):
                at = 256 + 128 * k
                mn = [own[2 * x + b, at : at + 128] for b in range(2)]
                ot = [other[2 * x + b, at : at + 128] for b in range(2)]
                for c in range(2):
                    a, b = (mn, ot) if c == 0 else (ot, mn)
                    line = [jnp.where(mine, a[i], b[i]) for i in range(2)]
                    col = 256 * x + 128 * c
                    keep[k, :, col : col + 128] = jnp.where(even, line[0], line[1])
                    send[k, :, col : col + 128] = jnp.where(even, line[1], line[0])

    return kernel(body, ((2, 128, 1024), (2, 128, 1024)))(own, other)


def down_call(layer, own, other, keep, send):
    def body(own, other, keep, send, out):
        act = jnp.dot(own[...], keep[layer], preferred_element_type=f32)
        act = act + jnp.dot(other[...], send[layer], preferred_element_type=f32)
        out[...] = act.astype(bf16)

    return kernel(body, ((256, 1024),))(own, other, keep, send)[0]


def step(prompt, norm_gain, gate_weight, up_weight, down_weight):
    gain = norm_gain[:, :, None]
    gate = (gain * gate_weight).astype(bf16)
    up = (gain * up_weight).astype(bf16)
    high = lax.axis_index("gr") == 1
    moved = []
    for layer in range(2):
        block = jnp.concatenate([gate[layer], up[layer]], axis=0)
        moved.append([lax.ppermute(block, AXES, weight_moves(k)) for k in range(2)])
    down = down_weight.astype(bf16).reshape(256, 128)
    across = lax.ppermute(down, "gr", SWAP)
    downs = in_order(down, across, high)
    rows = in_order(*moved[0], high)
    own = halves_to_all([jnp.concatenate([*columns(rows, b), downs[b]]) for b in range(2)])
    own, *late = lax.optimization_barrier((own, *moved[1]))
    rows = in_order(*late, high)
    early = own, lax.ppermute(own, "core", SWAP)
    own = halves_to_all([jnp.concatenate(columns(rows, b)) for b in range(2)])
    late = own, lax.ppermute(own, "core", SWAP)
    keep, send = down_rows_call(*early)
    came = lax.ppermute(send, "yl", SWAP)

    stream = prompt[0]
    yl = lax.axis_index("yl")
    mine = lax.dynamic_slice(
        stream, (lax.axis_index(("zl", "yh")) * 16, yl * 1024), (16, 1024)
    ).astype(f32)
    gates, ups = [], []
    for layer in range(2):
        gate, up, hidden = up_call(layer == 1, stream, *(late if layer else early))
        gates.append(gate)
        ups.append(up)
        other = lax.ppermute(hidden, "yl", SWAP)
        part = down_call(layer, hidden, other, keep, send)
        parts = lax.all_to_all(part.reshape(16, 16, 1024), ("zl", "yh"), 0, 0, tiled=True)
        mine = mine + 0.5 * jnp.sum(parts.astype(f32), axis=0)
        sends = jnp.broadcast_to(mine.astype(bf16)[None], (32, 16, 1024))
        stream = lax.all_to_all(sends, ("yl", "zl", "yh"), 0, 0, tiled=True)
        stream = stream.reshape(2, 256, 1024)
    mixed = jnp.concatenate(list(stream), axis=1)
    served = jnp.concatenate(in_order(keep, came, yl == 1), axis=2)
    return jnp.stack(gates), jnp.stack(ups), served, mixed[None]


def solution(mesh):
    fine = Mesh(mesh.devices.reshape(SIZES), AXES)
    in_specs = (P(GT, None, None), P(None, FS), P(None, FS, GT), P(None, FS, GT), P(None, FS, GT))
    out_specs = (P(None, None, FS), P(None, None, FS), P(None, FS, None), P(GT, None, None))
    return jax.shard_map(step, mesh=fine, in_specs=in_specs, out_specs=out_specs, check_vma=False)
```

```python
import jax
import jax.numpy as jnp
from jax import lax
from jax.experimental import pallas as pl
from jax.experimental.pallas import tpu as pltpu
from jax.sharding import Mesh
from jax.sharding import PartitionSpec as P


norm_eps = 1e-06
bf16 = jnp.bfloat16
f32 = jnp.float32

AXES = ("gr", "zl", "yh", "yl", "x", "core")
SIZES = (2, 4, 4, 2, 4, 2)
FS = ("zl", "yh", "yl")
GT = ("gr", "x", "core")
SWAP = [(0, 1), (1, 0)]


def device(gr, fs, tp):
    return gr * 256 + fs * 8 + tp


def everyone():
    return [(gr, fs, tp) for gr in range(2) for fs in range(32) for tp in range(8)]


def weight_moves():
    moves = []
    for gr, fs, tp in everyone():
        to = device(fs >> 4, 2 * (8 * gr + tp) + (fs & 1), (fs >> 1) & 7)
        moves.append((device(gr, fs, tp), to))
    return moves


def in_vmem(value):
    return pltpu.with_memory_space_constraint(value, pltpu.VMEM)


def kernel(body, outs, scratch=()):
    here = pl.BlockSpec(memory_space=pltpu.VMEM)

    def call(*args):
        return pl.pallas_call(
            body,
            in_specs=[here] * len(args),
            out_specs=tuple(here for _ in outs),
            out_shape=tuple(pltpu.VMEM(shape, bf16) for shape in outs),
            scratch_shapes=[pltpu.VMEM(shape, bf16) for shape in scratch],
            compiler_params=pltpu.CompilerParams(vmem_limit_bytes=16 << 20),
        )(*[in_vmem(a) for a in args])

    return call


def in_order(first, second, swapped):
    return jnp.where(swapped, second, first), jnp.where(swapped, first, second)


def halves_to_all(blocks):
    rows = blocks[0].shape[0]
    sends = jnp.broadcast_to(jnp.stack(blocks)[None], (4, 2, rows, 128)).reshape(8, rows, 128)
    return lax.all_to_all(sends, ("x", "yl"), 0, 0, tiled=True)


def columns(rows, b):
    return [r[:, 128 * b : 128 * b + 128] for r in rows]


def gather_rows(core, own, other, both):
    mine = core == 0
    for x in range(4):
        for b in range(2):
            for s in range(2):
                mn = own[2 * x + b, 128 * s : 128 * s + 128]
                ot = other[2 * x + b, 128 * s : 128 * s + 128]
                for c in range(2):
                    line = jnp.where(mine, mn, ot) if c == 0 else jnp.where(mine, ot, mn)
                    at = 64 * (16 * s + 4 * x + 2 * c + b)
                    both[at : at + 64, :128] = line[:64]
                    both[at : at + 64, 128:] = line[64:]


def up_call(late, stream, own, other):
    def body(stream, own, other, gate, up, hidden, both):
        gather_rows(lax.axis_index("core"), own, other, both)
        gate[...] = both[:, :128]
        up[...] = both[:, 128:]
        if late:
            squares = jnp.zeros((256, 1), f32)
            for z in range(4):
                part = stream[z // 2, :, 512 * (z % 2) : 512 * (z % 2) + 512].astype(f32)
                squares = squares + jnp.sum(part * part, axis=1, keepdims=True)
            scale = lax.rsqrt(squares * (1.0 / 2048) + norm_eps)
            act = jnp.zeros((256, 256), f32)
            for z in range(4):
                part = stream[z // 2, :, 512 * (z % 2) : 512 * (z % 2) + 512].astype(f32)
                part = (part * scale).astype(bf16)
                act = act + jnp.dot(part, both[512 * z : 512 * z + 512], preferred_element_type=f32)
        else:
            act = jnp.dot(stream[...], both[...], preferred_element_type=f32)
        gate_act, up_act = act[:, :128], act[:, 128:]
        hidden[...] = (gate_act / (1.0 + jnp.exp(-gate_act)) * up_act).astype(bf16)

    outs = ((2048, 128), (2048, 128), (256, 128))
    return kernel(body, outs, ((2048, 256),))(stream, own, other)


def norm_call(stream):
    def body(stream, out):
        value = stream[...].astype(f32)
        mean = jnp.sum(value * value, axis=1, keepdims=True) * (1.0 / 2048)
        out[...] = (value * lax.rsqrt(mean + norm_eps)).astype(bf16)

    return kernel(body, ((256, 2048),))(stream)[0]


def down_rows_call(own, other):
    def body(own, other, keep, send):
        mine = lax.axis_index("core") == 0
        even = lax.axis_index("yl") == 0
        for x in range(4):
            for k in range(2):
                at = 256 + 128 * k
                mn = [own[2 * x + b, at : at + 128] for b in range(2)]
                ot = [other[2 * x + b, at : at + 128] for b in range(2)]
                for c in range(2):
                    a, b = (mn, ot) if c == 0 else (ot, mn)
                    line = [jnp.where(mine, a[i], b[i]) for i in range(2)]
                    col = 256 * x + 128 * c
                    keep[k, :, col : col + 128] = jnp.where(even, line[0], line[1])
                    send[k, :, col : col + 128] = jnp.where(even, line[1], line[0])

    return kernel(body, ((2, 128, 1024), (2, 128, 1024)))(own, other)


def down_call(layer, own, other, keep, send):
    def body(own, other, keep, send, out):
        act = jnp.dot(own[...], keep[layer], preferred_element_type=f32)
        act = act + jnp.dot(other[...], send[layer], preferred_element_type=f32)
        out[...] = act.astype(bf16)

    return kernel(body, ((256, 1024),))(own, other, keep, send)[0]


def step(prompt, norm_gain, gate_weight, up_weight, down_weight):
    gain = norm_gain[:, :, None]
    gate = (gain * gate_weight).astype(bf16)
    up = (gain * up_weight).astype(bf16)
    high = lax.axis_index("gr") == 1
    moved = []
    for layer in range(2):
        block = jnp.concatenate([gate[layer], up[layer]], axis=0)
        moved.append(lax.ppermute(block, AXES, weight_moves()))
    down = down_weight.astype(bf16)
    down = jnp.concatenate([down[0], down[1]], axis=1)
    both = jnp.concatenate([moved[0], down], axis=0)
    across = lax.ppermute(both, "gr", SWAP)
    rows = in_order(both, across, high)
    blocks = []
    for b in range(2):
        lower = [rows[b][128:, :128], rows[b][128:, 128:]]
        blocks.append(jnp.concatenate([*columns([r[:128] for r in rows], b), *lower]))
    own = halves_to_all(blocks)
    across = lax.ppermute(moved[1], "gr", SWAP)
    own, *late = lax.optimization_barrier((own, moved[1], across))
    rows = in_order(*late, high)
    early = own, lax.ppermute(own, "core", SWAP)
    own = halves_to_all([jnp.concatenate(columns(rows, b)) for b in range(2)])
    late = own, lax.ppermute(own, "core", SWAP)
    keep, send = down_rows_call(*early)
    came = lax.ppermute(send, "yl", SWAP)

    stream = norm_call(prompt[0])
    yl = lax.axis_index("yl")
    mine = lax.dynamic_slice(
        prompt[0], (lax.axis_index(("zl", "yh")) * 16, yl * 1024), (16, 1024)
    ).astype(f32)
    gates, ups = [], []
    for layer in range(2):
        gate, up, hidden = up_call(layer == 1, stream, *(late if layer else early))
        gates.append(gate)
        ups.append(up)
        other = lax.ppermute(hidden, "yl", SWAP)
        part = down_call(layer, hidden, other, keep, send)
        parts = lax.all_to_all(part.reshape(16, 16, 1024), ("zl", "yh"), 0, 0, tiled=True)
        mine = mine + 0.5 * jnp.sum(parts.astype(f32), axis=0)
        sends = jnp.broadcast_to(mine.astype(bf16)[None], (32, 16, 1024))
        stream = lax.all_to_all(sends, ("yl", "zl", "yh"), 0, 0, tiled=True)
        stream = stream.reshape(2, 256, 1024)
    mixed = jnp.concatenate(list(stream), axis=1)
    served = jnp.concatenate(in_order(keep, came, yl == 1), axis=2)
    return jnp.stack(gates), jnp.stack(ups), served, mixed[None]


def solution(mesh):
    fine = Mesh(mesh.devices.reshape(SIZES), AXES)
    in_specs = (P(GT, None, None), P(None, FS), P(None, FS, GT), P(None, FS, GT), P(None, FS, GT))
    out_specs = (P(None, None, FS), P(None, None, FS), P(None, FS, None), P(GT, None, None))
    return jax.shard_map(step, mesh=fine, in_specs=in_specs, out_specs=out_specs, check_vma=False)
```

```python
import jax
import jax.numpy as jnp
from jax import lax
from jax.experimental import pallas as pl
from jax.experimental.pallas import tpu as pltpu
from jax.sharding import Mesh
from jax.sharding import PartitionSpec as P


norm_eps = 1e-06
bf16 = jnp.bfloat16
f32 = jnp.float32

AXES = ("gr", "zl", "yh", "yl", "x", "core")
SIZES = (2, 4, 4, 2, 4, 2)
FS = ("zl", "yh", "yl")
GT = ("gr", "x", "core")
SWAP = [(0, 1), (1, 0)]


def device(gr, fs, tp):
    return gr * 256 + fs * 8 + tp


def everyone():
    return [(gr, fs, tp) for gr in range(2) for fs in range(32) for tp in range(8)]


def weight_moves():
    moves = []
    for gr, fs, tp in everyone():
        to = device(fs >> 4, 2 * (8 * gr + tp) + (fs & 1), (fs >> 1) & 7)
        moves.append((device(gr, fs, tp), to))
    return moves


def in_vmem(value):
    return pltpu.with_memory_space_constraint(value, pltpu.VMEM)


def kernel(body, outs, scratch=()):
    here = pl.BlockSpec(memory_space=pltpu.VMEM)

    def call(*args):
        return pl.pallas_call(
            body,
            in_specs=[here] * len(args),
            out_specs=tuple(here for _ in outs),
            out_shape=tuple(pltpu.VMEM(shape, bf16) for shape in outs),
            scratch_shapes=[pltpu.VMEM(shape, bf16) for shape in scratch],
            compiler_params=pltpu.CompilerParams(vmem_limit_bytes=16 << 20),
        )(*[in_vmem(a) for a in args])

    return call


def in_order(first, second, swapped):
    return jnp.where(swapped, second, first), jnp.where(swapped, first, second)


def to_everyone(value, axes, count):
    return lax.all_to_all(
        jnp.broadcast_to(value[None], (count, *value.shape)), axes, 0, 0, tiled=True
    )


def halves_to_all(blocks):
    rows = blocks[0].shape[0]
    sends = jnp.broadcast_to(jnp.stack(blocks)[None], (4, 2, rows, 128)).reshape(8, rows, 128)
    return lax.all_to_all(sends, ("x", "yl"), 0, 0, tiled=True)


def columns(rows, b):
    return [r[:, 128 * b : 128 * b + 128] for r in rows]


def gather_rows(core, own, other, both):
    mine = core == 0
    width = both.shape[1] // 2
    for x in range(4):
        for b in range(2):
            for s in range(2):
                mn = own[2 * x + b, 128 * s : 128 * s + 128]
                ot = other[2 * x + b, 128 * s : 128 * s + 128]
                for c in range(2):
                    line = jnp.where(mine, mn, ot) if c == 0 else jnp.where(mine, ot, mn)
                    at = 64 * (16 * s + 4 * x + 2 * c + b)
                    both[at : at + 64, :width] = line[:64]
                    both[at : at + 64, width:] = line[64:]


def gated(act):
    width = act.shape[1] // 2
    gate_act, up_act = act[:, :width], act[:, width:]
    return (gate_act / (1.0 + jnp.exp(-gate_act)) * up_act).astype(bf16)


def early_up_call(normed, own, other):
    def body(normed, own, other, gate, up, hidden, both):
        gather_rows(lax.axis_index("core"), own, other, both)
        gate[...] = both[:, :128]
        up[...] = both[:, 128:]
        hidden[...] = gated(jnp.dot(normed[...], both[...], preferred_element_type=f32))

    outs = ((2048, 128), (2048, 128), (256, 128))
    return kernel(body, outs, ((2048, 256),))(normed, own, other)


def late_up_call(stream, own, other):
    def body(stream, own, other, gate, up, hidden, both):
        gather_rows(lax.axis_index("core"), own, other, both)
        even = lax.axis_index("yl") == 0
        gate[...] = jnp.where(even, both[:, :128], both[:, 128:256])
        up[...] = jnp.where(even, both[:, 256:384], both[:, 384:])
        squares = jnp.zeros((128, 1), f32)
        for z in range(2):
            part = stream[z].astype(f32)
            squares = squares + jnp.sum(part * part, axis=1, keepdims=True)
        scale = lax.rsqrt(squares * (1.0 / 2048) + norm_eps)
        act = jnp.zeros((128, 512), f32)
        for z in range(2):
            part = (stream[z].astype(f32) * scale).astype(bf16)
            rows = both[1024 * z : 1024 * z + 1024]
            act = act + jnp.dot(part, rows, preferred_element_type=f32)
        hidden[...] = gated(act)

    outs = ((2048, 128), (2048, 128), (128, 256))
    return kernel(body, outs, ((2048, 512),))(stream, own, other)


def norm_call(stream):
    def body(stream, out):
        value = stream[...].astype(f32)
        mean = jnp.sum(value * value, axis=1, keepdims=True) * (1.0 / 2048)
        out[...] = (value * lax.rsqrt(mean + norm_eps)).astype(bf16)

    return kernel(body, ((256, 2048),))(stream)[0]


def down_rows_call(own, other):
    def body(own, other, keep, send, pair, one):
        mine = lax.axis_index("core") == 0
        even = lax.axis_index("yl") == 0
        for x in range(4):
            for k in range(3):
                at = 256 + 128 * k
                mn = [own[2 * x + b, at : at + 128] for b in range(2)]
                ot = [other[2 * x + b, at : at + 128] for b in range(2)]
                for c in range(2):
                    a, b = (mn, ot) if c == 0 else (ot, mn)
                    line = [jnp.where(mine, a[i], b[i]) for i in range(2)]
                    col = 256 * x + 128 * c
                    if k == 0:
                        keep[:, col : col + 128] = jnp.where(even, line[0], line[1])
                        send[:, col : col + 128] = jnp.where(even, line[1], line[0])
                    else:
                        col = col + 1024 * (k - 1)
                        one[:, col : col + 128] = jnp.where(even, line[0], line[1])
                        pair[:128, col : col + 128] = line[0]
                        pair[128:, col : col + 128] = line[1]

    outs = ((128, 1024), (128, 1024), (256, 2048), (128, 2048))
    return kernel(body, outs)(own, other)


def early_down_call(own, other, keep, send):
    def body(own, other, keep, send, out):
        act = jnp.dot(own[...], keep[...], preferred_element_type=f32)
        act = act + jnp.dot(other[...], send[...], preferred_element_type=f32)
        out[...] = act.astype(bf16)

    return kernel(body, ((256, 1024),))(own, other, keep, send)[0]


def late_down_call(hidden, pair):
    def body(hidden, pair, out):
        out[...] = jnp.dot(hidden[...], pair[...], preferred_element_type=f32).astype(bf16)

    return kernel(body, ((128, 2048),))(hidden, pair)[0]


def step(prompt, norm_gain, gate_weight, up_weight, down_weight):
    gain = norm_gain[:, :, None]
    gate = (gain * gate_weight).astype(bf16)
    up = (gain * up_weight).astype(bf16)
    high = lax.axis_index("gr") == 1
    moved = []
    for layer in range(2):
        block = jnp.concatenate([gate[layer], up[layer]], axis=0)
        moved.append(lax.ppermute(block, AXES, weight_moves()))
    down = down_weight.astype(bf16)
    down = jnp.concatenate([down[0], down[1]], axis=1)
    both = jnp.concatenate([moved[0], down], axis=0)
    across = lax.ppermute(both, "gr", SWAP)
    rows = in_order(both, across, high)
    blocks = []
    for b in range(2):
        lower = [rows[b][128:, :128], rows[0][128:, 128:], rows[1][128:, 128:]]
        blocks.append(jnp.concatenate([*columns([r[:128] for r in rows], b), *lower]))
    own = halves_to_all(blocks)
    across = lax.ppermute(moved[1], "gr", SWAP)
    own, *late = lax.optimization_barrier((own, moved[1], across))
    rows = in_order(*late, high)
    early = own, lax.ppermute(own, "core", SWAP)
    own = to_everyone(jnp.concatenate(rows), ("x", "yl"), 8)
    late = own, lax.ppermute(own, "core", SWAP)
    keep, send, pair, one = down_rows_call(*early)
    came = lax.ppermute(send, "yl", SWAP)

    yl = lax.axis_index("yl")
    odd = yl == 1
    normed = norm_call(prompt[0])
    gate0, up0, hidden = early_up_call(normed, *early)
    other = lax.ppermute(hidden, "yl", SWAP)
    part = early_down_call(hidden, other, keep, send)
    parts = lax.all_to_all(part.reshape(16, 16, 1024), ("zl", "yh"), 0, 0, tiled=True)
    start = lax.axis_index(("zl", "yh")) * 16, yl * 1024
    mine = lax.dynamic_slice(prompt[0], start, (16, 1024)).astype(f32)
    mine = mine + 0.5 * jnp.sum(parts.astype(f32), axis=0)
    sends = mine.astype(bf16).reshape(2, 1, 8, 1024)
    sends = jnp.broadcast_to(sends, (2, 16, 8, 1024)).reshape(32, 8, 1024)
    stream = lax.all_to_all(sends, ("yl", "zl", "yh"), 0, 0, tiled=True)
    kept, sent = in_order(mine[:8], mine[8:], odd)
    rest = lax.ppermute(sent, "yl", SWAP)
    mine = jnp.concatenate(in_order(kept, rest, odd), axis=1)
    gate1, up1, hidden = late_up_call(stream.reshape(2, 128, 1024), *late)
    part = late_down_call(hidden, pair)
    parts = lax.all_to_all(part.reshape(16, 8, 2048), ("zl", "yh"), 0, 0, tiled=True)
    mine = mine + 0.5 * jnp.sum(parts.astype(f32), axis=0)
    mixed = to_everyone(mine.astype(bf16), FS, 32)
    served = jnp.stack([jnp.concatenate(in_order(keep, came, odd), axis=1), one])
    gates, ups = jnp.stack([gate0, gate1]), jnp.stack([up0, up1])
    return gates, ups, served, mixed.reshape(prompt.shape)


def solution(mesh):
    fine = Mesh(mesh.devices.reshape(SIZES), AXES)
    in_specs = (P(GT, None, None), P(None, FS), P(None, FS, GT), P(None, FS, GT), P(None, FS, GT))
    out_specs = (P(None, None, FS), P(None, None, FS), P(None, FS, None), P(GT, None, None))
    return jax.shard_map(step, mesh=fine, in_specs=in_specs, out_specs=out_specs, check_vma=False)
```

```python
import jax
import jax.numpy as jnp
from jax import lax
from jax.experimental import pallas as pl
from jax.experimental.pallas import tpu as pltpu
from jax.sharding import Mesh
from jax.sharding import PartitionSpec as P


norm_eps = 1e-06
bf16 = jnp.bfloat16
f32 = jnp.float32

AXES = ("gr", "zl", "yh", "yl", "x", "core")
SIZES = (2, 4, 4, 2, 4, 2)
FS = ("zl", "yh", "yl")
GT = ("gr", "x", "core")
SWAP = [(0, 1), (1, 0)]


def device(gr, fs, tp):
    return gr * 256 + fs * 8 + tp


def everyone():
    return [(gr, fs, tp) for gr in range(2) for fs in range(32) for tp in range(8)]


def weight_moves():
    moves = []
    for gr, fs, tp in everyone():
        to = device(fs >> 4, 2 * (8 * gr + tp) + (fs & 1), (fs >> 1) & 7)
        moves.append((device(gr, fs, tp), to))
    return moves


def in_vmem(value):
    return pltpu.with_memory_space_constraint(value, pltpu.VMEM)


def kernel(body, outs, scratch=()):
    here = pl.BlockSpec(memory_space=pltpu.VMEM)

    def call(*args):
        return pl.pallas_call(
            body,
            in_specs=[here] * len(args),
            out_specs=tuple(here for _ in outs),
            out_shape=tuple(pltpu.VMEM(shape, bf16) for shape in outs),
            scratch_shapes=[pltpu.VMEM(shape, bf16) for shape in scratch],
            compiler_params=pltpu.CompilerParams(vmem_limit_bytes=24 << 20),
        )(*[in_vmem(a) for a in args])

    return call


def in_order(first, second, swapped):
    return jnp.where(swapped, second, first), jnp.where(swapped, first, second)


def to_everyone(value, axes, count):
    return lax.all_to_all(
        jnp.broadcast_to(value[None], (count, *value.shape)), axes, 0, 0, tiled=True
    )


def layer_call(late, normed, own, other):
    def body(normed, own, other, gate, up, served, part, wide, down):
        core = lax.axis_index("core") == 0
        even = lax.axis_index("yl") == 0
        for k in range(4):
            x = lax.axis_index("x") ^ k if late else k
            for b in range(2):
                for s in range(3):
                    mn = own[k, b, 128 * s : 128 * s + 128]
                    ot = other[k, b, 128 * s : 128 * s + 128]
                    for c in range(2):
                        line = jnp.where(core, mn, ot) if c == 0 else jnp.where(core, ot, mn)
                        at = 128 * c + 64 * b
                        if s < 2:
                            wide[s, x, at : at + 64, :256] = line[:64]
                            wide[s, x, at : at + 64, 256:] = line[64:]
                        else:
                            for g in range(2):
                                down[g, x, 128 * b : 128 * b + 128, 128 * c : 128 * c + 128] = line[
                                    :, 128 * g : 128 * g + 128
                                ]
        act = jnp.zeros((128, 512), f32)
        for s in range(2):
            for x in range(4):
                at = 1024 * s + 256 * x
                block = wide[s, x]
                gate[at : at + 256] = jnp.where(even, block[:, :128], block[:, 128:256])
                up[at : at + 256] = jnp.where(even, block[:, 256:384], block[:, 384:])
                act = act + jnp.dot(normed[:, at : at + 256], block, preferred_element_type=f32)
        gate_act, up_act = act[:, :256], act[:, 256:]
        hidden = (gate_act / (1.0 + jnp.exp(-gate_act)) * up_act).astype(bf16)
        for g in range(2):
            for x in range(4):
                at = 1024 * g + 256 * x
                block = down[g, x]
                served[:, at : at + 256] = jnp.where(even, block[:128], block[128:])
                out = jnp.dot(hidden, block, preferred_element_type=f32)
                part[:, at : at + 256] = out.astype(bf16)

    outs = ((2048, 128), (2048, 128), (128, 2048), (128, 2048))
    scratch = ((2, 4, 256, 512), (2, 4, 256, 256))
    return kernel(body, outs, scratch)(normed, own, other)


def normalised(value):
    mean = jnp.sum(value * value, axis=1, keepdims=True) * (1.0 / 2048)
    return (value * lax.rsqrt(mean + norm_eps)).astype(bf16)


def norm_call(stream):
    def body(stream, out):
        out[...] = normalised(stream[...].astype(f32))

    return kernel(body, (stream.shape,))(stream)[0]


def step(prompt, norm_gain, gate_weight, up_weight, down_weight):
    gain = norm_gain[:, :, None]
    gate = (gain * gate_weight).astype(bf16)
    up = (gain * up_weight).astype(bf16)
    high = lax.axis_index("gr") == 1
    moved = []
    for layer in range(2):
        block = jnp.concatenate([gate[layer], up[layer]], axis=0)
        moved.append(lax.ppermute(block, AXES, weight_moves()))
    down = down_weight.astype(bf16)
    both = jnp.concatenate([moved[0], jnp.concatenate([down[0], down[1]], axis=1)], axis=0)
    across = lax.ppermute(both, "gr", SWAP)
    low, top = in_order(both, across, high)

    def downs(layer):
        cols = slice(128 * layer, 128 * layer + 128)
        return jnp.concatenate([low[128:, cols], top[128:, cols]], axis=1)

    block = jnp.concatenate([low[:128], top[:128], downs(0)], axis=0)
    own = to_everyone(block, ("x", "yl"), 8)
    across = lax.ppermute(moved[1], "gr", SWAP)
    block = jnp.concatenate([*in_order(moved[1], across, high), downs(1)], axis=0)
    yl = lax.axis_index("yl")
    came = lax.ppermute(block, "yl", SWAP)
    own, block = lax.optimization_barrier((own, block))
    other = lax.ppermute(own, "core", SWAP)
    pair = jnp.stack(in_order(block, came, yl == 1))
    late = [lax.ppermute(pair, "x", [(x, x ^ k) for x in range(4)]) for k in (1, 2, 3)]
    late = jnp.stack([pair, *late])
    late_other = lax.ppermute(late, "core", SWAP)

    half = lax.dynamic_slice_in_dim(prompt[0], yl * 128, 128, 0)
    mine = lax.dynamic_slice_in_dim(half, lax.axis_index(("zl", "yh")) * 8, 8, 0).astype(f32)
    normed = norm_call(half)
    early = [a.reshape(4, 2, 384, 256) for a in (own, other)]
    gates, ups, served = [], [], []
    for layer in range(2):
        pieces = (late, late_other) if layer else early
        gate, up, down, part = layer_call(layer == 1, normed, *pieces)
        gates.append(gate)
        ups.append(up)
        served.append(down)
        parts = lax.all_to_all(part.reshape(16, 8, 2048), ("zl", "yh"), 0, 0, tiled=True)
        mine = mine + 0.5 * jnp.sum(parts.astype(f32), axis=0)
        if layer == 0:
            normed = to_everyone(normalised(mine), ("zl", "yh"), 16).reshape(128, 2048)
        else:
            mixed = to_everyone(mine.astype(bf16), ("yl", "zl", "yh"), 32)
    return jnp.stack(gates), jnp.stack(ups), jnp.stack(served), mixed.reshape(prompt.shape)


def solution(mesh):
    fine = Mesh(mesh.devices.reshape(SIZES), AXES)
    in_specs = (P(GT, None, None), P(None, FS), P(None, FS, GT), P(None, FS, GT), P(None, FS, GT))
    out_specs = (P(None, None, FS), P(None, None, FS), P(None, FS, None), P(GT, None, None))
    return jax.shard_map(step, mesh=fine, in_specs=in_specs, out_specs=out_specs, check_vma=False)
```

```python
import jax
import jax.numpy as jnp
from jax import lax
from jax.experimental import pallas as pl
from jax.experimental.pallas import tpu as pltpu
from jax.sharding import Mesh
from jax.sharding import PartitionSpec as P


norm_eps = 1e-06
bf16 = jnp.bfloat16
f32 = jnp.float32

AXES = ("gr", "zl", "yh", "yl", "x", "core")
SIZES = (2, 4, 4, 2, 4, 2)
FS = ("zl", "yh", "yl")
GT = ("gr", "x", "core")
SWAP = [(0, 1), (1, 0)]


def device(gr, fs, tp):
    return gr * 256 + fs * 8 + tp


def everyone():
    return [(gr, fs, tp) for gr in range(2) for fs in range(32) for tp in range(8)]


def weight_moves():
    moves = []
    for gr, fs, tp in everyone():
        to = device(fs >> 4, 2 * (8 * gr + tp) + (fs & 1), (fs >> 1) & 7)
        moves.append((device(gr, fs, tp), to))
    return moves


def in_vmem(value):
    return pltpu.with_memory_space_constraint(value, pltpu.VMEM)


def kernel(body, outs, scratch=()):
    here = pl.BlockSpec(memory_space=pltpu.VMEM)

    def call(*args):
        return pl.pallas_call(
            body,
            in_specs=[here] * len(args),
            out_specs=tuple(here for _ in outs),
            out_shape=tuple(pltpu.VMEM(shape, bf16) for shape in outs),
            scratch_shapes=[pltpu.VMEM(shape, bf16) for shape in scratch],
            compiler_params=pltpu.CompilerParams(vmem_limit_bytes=24 << 20),
        )(*[in_vmem(a) for a in args])

    return call


def in_order(first, second, swapped):
    return jnp.where(swapped, second, first), jnp.where(swapped, first, second)


def to_everyone(value, axes, count):
    return lax.all_to_all(
        jnp.broadcast_to(value[None], (count, *value.shape)), axes, 0, 0, tiled=True
    )


def layer_call(late, normed, own, other):
    def body(normed, own, other, gate, up, served, part, wide, down):
        core = lax.axis_index("core") == 0
        even = lax.axis_index("yl") == 0
        for k in range(4):
            x = lax.axis_index("x") ^ k if late else k
            for b in range(2):
                for s in range(3):
                    mn = own[k, b, 128 * s : 128 * s + 128]
                    ot = other[k, b, 128 * s : 128 * s + 128]
                    for c in range(2):
                        line = jnp.where(core, mn, ot) if c == 0 else jnp.where(core, ot, mn)
                        at = 128 * c + 64 * b
                        if s < 2:
                            wide[s, x, at : at + 64, :256] = line[:64]
                            wide[s, x, at : at + 64, 256:] = line[64:]
                        else:
                            for g in range(2):
                                down[g, x, 128 * b : 128 * b + 128, 128 * c : 128 * c + 128] = line[
                                    :, 128 * g : 128 * g + 128
                                ]
        act = jnp.zeros((128, 512), f32)
        for s in range(2):
            for x in range(4):
                at = 1024 * s + 256 * x
                block = wide[s, x]
                gate[at : at + 256] = jnp.where(even, block[:, :128], block[:, 128:256])
                up[at : at + 256] = jnp.where(even, block[:, 256:384], block[:, 384:])
                act = act + jnp.dot(normed[:, at : at + 256], block, preferred_element_type=f32)
        gate_act, up_act = act[:, :256], act[:, 256:]
        hidden = (gate_act / (1.0 + jnp.exp(-gate_act)) * up_act).astype(bf16)
        for g in range(2):
            for x in range(4):
                at = 1024 * g + 256 * x
                block = down[g, x]
                served[:, at : at + 256] = jnp.where(even, block[:128], block[128:])
                out = jnp.dot(hidden, block, preferred_element_type=f32)
                part[:, at : at + 256] = out.astype(bf16)

    outs = ((2048, 128), (2048, 128), (128, 2048), (128, 2048))
    scratch = ((2, 4, 256, 512), (2, 4, 256, 256))
    return kernel(body, outs, scratch)(normed, own, other)


def normalised(value):
    mean = jnp.sum(value * value, axis=1, keepdims=True) * (1.0 / 2048)
    return (value * lax.rsqrt(mean + norm_eps)).astype(bf16)


def norm_call(stream):
    def body(stream, out):
        out[...] = normalised(stream[...].astype(f32))

    return kernel(body, (stream.shape,))(stream)[0]


def fold_call(last, parts, mine):
    count = 32 if last else 16

    def body(parts, mine, sends, total):
        value = mine[...]
        summed = parts[0].astype(f32)
        for i in range(1, 16):
            summed = summed + parts[i].astype(f32)
        value = value + 0.5 * summed
        total[...] = value
        sent = value.astype(bf16) if last else normalised(value)
        for i in range(count):
            sends[i] = sent

    here = pl.BlockSpec(memory_space=pltpu.VMEM)
    return pl.pallas_call(
        body,
        in_specs=[here, here],
        out_specs=(here, here),
        out_shape=(pltpu.VMEM((count, 8, 2048), bf16), pltpu.VMEM((8, 2048), f32)),
        compiler_params=pltpu.CompilerParams(vmem_limit_bytes=24 << 20),
        name="fold",
    )(in_vmem(parts), in_vmem(mine))


def step(prompt, norm_gain, gate_weight, up_weight, down_weight):
    gain = norm_gain[:, :, None]
    gate = (gain * gate_weight).astype(bf16)
    up = (gain * up_weight).astype(bf16)
    high = lax.axis_index("gr") == 1
    moved = []
    for layer in range(2):
        block = jnp.concatenate([gate[layer], up[layer]], axis=0)
        moved.append(lax.ppermute(block, AXES, weight_moves()))
    down = down_weight.astype(bf16)

    def with_down(layer):
        packed = jnp.concatenate([down[layer, :64], down[layer, 64:]], axis=1)
        return jnp.concatenate([moved[layer], packed], axis=0)

    def unpacked(low, top):
        upper = jnp.concatenate([low[128:, :128], top[128:, :128]], axis=1)
        lower = jnp.concatenate([low[128:, 128:], top[128:, 128:]], axis=1)
        return jnp.concatenate([low[:128], top[:128], upper, lower], axis=0)

    both = with_down(0)
    across = lax.ppermute(both, "gr", SWAP)
    block = unpacked(*in_order(both, across, high))

    own = to_everyone(block, ("x", "yl"), 8)
    both = with_down(1)
    across = lax.ppermute(both, "gr", SWAP)
    block = unpacked(*in_order(both, across, high))
    yl = lax.axis_index("yl")
    came = lax.ppermute(block, "yl", SWAP)
    own, block = lax.optimization_barrier((own, block))
    other = lax.ppermute(own, "core", SWAP)
    pair = jnp.stack(in_order(block, came, yl == 1))
    late = [lax.ppermute(pair, "x", [(x, x ^ k) for x in range(4)]) for k in (1, 2, 3)]
    late = jnp.stack([pair, *late])
    late_other = lax.ppermute(late, "core", SWAP)

    half = lax.dynamic_slice_in_dim(prompt[0], yl * 128, 128, 0)
    mine = lax.dynamic_slice_in_dim(half, lax.axis_index(("zl", "yh")) * 8, 8, 0).astype(f32)
    normed = norm_call(half)
    early = [a.reshape(4, 2, 384, 256) for a in (own, other)]
    gates, ups, served = [], [], []
    for layer in range(2):
        pieces = (late, late_other) if layer else early
        gate, up, down, part = layer_call(layer == 1, normed, *pieces)
        gates.append(gate)
        ups.append(up)
        served.append(down)
        parts = lax.all_to_all(part.reshape(16, 8, 2048), ("zl", "yh"), 0, 0, tiled=True)
        sends, mine = fold_call(layer == 1, parts, mine)
        axes = ("yl", "zl", "yh") if layer else ("zl", "yh")
        normed = lax.all_to_all(sends, axes, 0, 0, tiled=True).reshape(-1, 2048)
    stacks = jnp.stack(gates), jnp.stack(ups), jnp.stack(served)
    return *stacks, normed.reshape(prompt.shape)


def solution(mesh):
    fine = Mesh(mesh.devices.reshape(SIZES), AXES)
    in_specs = (P(GT, None, None), P(None, FS), P(None, FS, GT), P(None, FS, GT), P(None, FS, GT))
    out_specs = (P(None, None, FS), P(None, None, FS), P(None, FS, None), P(GT, None, None))
    return jax.shard_map(step, mesh=fine, in_specs=in_specs, out_specs=out_specs, check_vma=False)
```

```python
import jax
import jax.numpy as jnp
from jax import lax
from jax.experimental import pallas as pl
from jax.experimental.pallas import tpu as pltpu
from jax.sharding import Mesh
from jax.sharding import PartitionSpec as P


norm_eps = 1e-06
bf16 = jnp.bfloat16
f32 = jnp.float32

AXES = ("gr", "zl", "yh", "yl", "x", "core")
SIZES = (2, 4, 4, 2, 4, 2)
FS = ("zl", "yh", "yl")
GT = ("gr", "x", "core")
SWAP = [(0, 1), (1, 0)]


def device(gr, fs, tp):
    return gr * 256 + fs * 8 + tp


def everyone():
    return [(gr, fs, tp) for gr in range(2) for fs in range(32) for tp in range(8)]


def weight_moves():
    moves = []
    for gr, fs, tp in everyone():
        to = device(fs >> 4, 2 * (8 * gr + tp) + (fs & 1), (fs >> 1) & 7)
        moves.append((device(gr, fs, tp), to))
    return moves


def in_vmem(value):
    return pltpu.with_memory_space_constraint(value, pltpu.VMEM)


def kernel(body, outs, scratch=()):
    here = pl.BlockSpec(memory_space=pltpu.VMEM)

    def call(*args):
        return pl.pallas_call(
            body,
            in_specs=[here] * len(args),
            out_specs=tuple(here for _ in outs),
            out_shape=tuple(pltpu.VMEM(shape, bf16) for shape in outs),
            scratch_shapes=[pltpu.VMEM(shape, bf16) for shape in scratch],
            compiler_params=pltpu.CompilerParams(vmem_limit_bytes=24 << 20),
        )(*[in_vmem(a) for a in args])

    return call


def in_order(first, second, swapped):
    return jnp.where(swapped, second, first), jnp.where(swapped, first, second)


def to_everyone(value, axes, count):
    return lax.all_to_all(
        jnp.broadcast_to(value[None], (count, *value.shape)), axes, 0, 0, tiled=True
    )


def layer_call(late, normed, own, other, outputs):
    layer = 1 if late else 0

    def body(normed, own, other, *refs):
        gates, ups, serveds, part, wide, down, gate, up, served, done = refs[3 * layer :]
        core = lax.axis_index("core") == 0
        even = lax.axis_index("yl") == 0
        for k in range(4):
            x = lax.axis_index("x") ^ k if late else k
            for b in range(2):
                for s in range(3):
                    mn = own[k, b, 128 * s : 128 * s + 128]
                    ot = other[k, b, 128 * s : 128 * s + 128]
                    for c in range(2):
                        line = jnp.where(core, mn, ot) if c == 0 else jnp.where(core, ot, mn)
                        at = 128 * c + 64 * b
                        if s < 2:
                            wide[s, x, at : at + 64, :256] = line[:64]
                            wide[s, x, at : at + 64, 256:] = line[64:]
                        else:
                            for g in range(2):
                                down[g, x, 128 * b : 128 * b + 128, 128 * c : 128 * c + 128] = line[
                                    :, 128 * g : 128 * g + 128
                                ]
        act = jnp.zeros((128, 512), f32)
        for s in range(2):
            for x in range(4):
                at = 1024 * s + 256 * x
                block = wide[s, x]
                gate[at : at + 256] = jnp.where(even, block[:, :128], block[:, 128:256])
                up[at : at + 256] = jnp.where(even, block[:, 256:384], block[:, 384:])
        for g in range(2):
            for x in range(4):
                block = down[g, x]
                at = 1024 * g + 256 * x
                served[:, at : at + 256] = jnp.where(even, block[:128], block[128:])
        copies = [
            pltpu.make_async_copy(a, b.at[layer], done.at[i])
            for i, (a, b) in enumerate(((gate, gates), (up, ups), (served, serveds)))
        ]
        for copy in copies:
            copy.start()
        for s in range(2):
            for x in range(4):
                at = 1024 * s + 256 * x
                act = act + jnp.dot(
                    normed[:, at : at + 256], wide[s, x], preferred_element_type=f32
                )
        gate_act, up_act = act[:, :256], act[:, 256:]
        hidden = (gate_act / (1.0 + jnp.exp(-gate_act)) * up_act).astype(bf16)
        for g in range(2):
            for x in range(4):
                at = 1024 * g + 256 * x
                out = jnp.dot(hidden, down[g, x], preferred_element_type=f32)
                part[:, at : at + 256] = out.astype(bf16)
        for copy in copies:
            copy.wait()

    here = pl.BlockSpec(memory_space=pltpu.VMEM)
    there = pl.BlockSpec(memory_space=pl.ANY)
    scratch = ((2, 4, 256, 512), (2, 4, 256, 256), (2048, 128), (2048, 128), (128, 2048))
    shapes = ((2, 2048, 128), (2, 2048, 128), (2, 128, 2048))
    return pl.pallas_call(
        body,
        in_specs=[here] * 3 + [there] * len(outputs),
        out_specs=(there, there, there, here),
        out_shape=(
            *(jax.ShapeDtypeStruct(shape, bf16) for shape in shapes),
            pltpu.VMEM((128, 2048), bf16),
        ),
        input_output_aliases={3 + i: i for i in range(len(outputs))},
        scratch_shapes=[
            *(pltpu.VMEM(shape, bf16) for shape in scratch),
            pltpu.SemaphoreType.DMA((3,)),
        ],
        compiler_params=pltpu.CompilerParams(vmem_limit_bytes=24 << 20),
        name="late_layer" if late else "early_layer",
    )(in_vmem(normed), in_vmem(own), in_vmem(other), *outputs)


def normalised(value):
    mean = jnp.sum(value * value, axis=1, keepdims=True) * (1.0 / 2048)
    return (value * lax.rsqrt(mean + norm_eps)).astype(bf16)


def norm_call(stream):
    def body(stream, out):
        out[...] = normalised(stream[...].astype(f32))

    return kernel(body, (stream.shape,))(stream)[0]


def fold_call(last, parts, mine):
    count = 32 if last else 16

    def body(parts, mine, sends, total):
        value = mine[...]
        summed = parts[0].astype(f32)
        for i in range(1, 16):
            summed = summed + parts[i].astype(f32)
        value = value + 0.5 * summed
        total[...] = value
        sent = value.astype(bf16) if last else normalised(value)
        for i in range(count):
            sends[i] = sent

    here = pl.BlockSpec(memory_space=pltpu.VMEM)
    return pl.pallas_call(
        body,
        in_specs=[here, here],
        out_specs=(here, here),
        out_shape=(pltpu.VMEM((count, 8, 2048), bf16), pltpu.VMEM((8, 2048), f32)),
        compiler_params=pltpu.CompilerParams(vmem_limit_bytes=24 << 20),
        name="fold",
    )(in_vmem(parts), in_vmem(mine))


def step(prompt, norm_gain, gate_weight, up_weight, down_weight):
    gain = norm_gain[:, :, None]
    gate = (gain * gate_weight).astype(bf16)
    up = (gain * up_weight).astype(bf16)
    high = lax.axis_index("gr") == 1
    moved = []
    for layer in range(2):
        block = jnp.concatenate([gate[layer], up[layer]], axis=0)
        moved.append(lax.ppermute(block, AXES, weight_moves()))
    down = down_weight.astype(bf16)

    def with_down(layer):
        packed = jnp.concatenate([down[layer, :64], down[layer, 64:]], axis=1)
        return jnp.concatenate([moved[layer], packed], axis=0)

    def unpacked(low, top):
        upper = jnp.concatenate([low[128:, :128], top[128:, :128]], axis=1)
        lower = jnp.concatenate([low[128:, 128:], top[128:, 128:]], axis=1)
        return jnp.concatenate([low[:128], top[:128], upper, lower], axis=0)

    both = with_down(0)
    across = lax.ppermute(both, "gr", SWAP)
    block = unpacked(*in_order(both, across, high))

    own = to_everyone(block, ("x", "yl"), 8)
    own, moved[1] = lax.optimization_barrier((own, moved[1]))
    both = with_down(1)
    across = lax.ppermute(both, "gr", SWAP)
    block = unpacked(*in_order(both, across, high))
    yl = lax.axis_index("yl")
    came = lax.ppermute(block, "yl", SWAP)
    other = lax.ppermute(own, "core", SWAP)
    pair = jnp.stack(in_order(block, came, yl == 1))
    late = [lax.ppermute(pair, "x", [(x, x ^ k) for x in range(4)]) for k in (1, 2, 3)]
    late = jnp.stack([pair, *late])
    late_other = lax.ppermute(late, "core", SWAP)

    half = lax.dynamic_slice_in_dim(prompt[0], yl * 128, 128, 0)
    mine = lax.dynamic_slice_in_dim(half, lax.axis_index(("zl", "yh")) * 8, 8, 0).astype(f32)
    normed = norm_call(half)
    early = [a.reshape(4, 2, 384, 256) for a in (own, other)]
    outputs = ()
    for layer in range(2):
        pieces = (late, late_other) if layer else early
        *outputs, part = layer_call(layer == 1, normed, *pieces, outputs)
        parts = lax.all_to_all(part.reshape(16, 8, 2048), ("zl", "yh"), 0, 0, tiled=True)
        sends, mine = fold_call(layer == 1, parts, mine)
        axes = ("yl", "zl", "yh") if layer else ("zl", "yh")
        normed = lax.all_to_all(sends, axes, 0, 0, tiled=True).reshape(-1, 2048)
    return *outputs, normed.reshape(prompt.shape)


def solution(mesh):
    fine = Mesh(mesh.devices.reshape(SIZES), AXES)
    in_specs = (P(GT, None, None), P(None, FS), P(None, FS, GT), P(None, FS, GT), P(None, FS, GT))
    out_specs = (P(None, None, FS), P(None, None, FS), P(None, FS, None), P(GT, None, None))
    return jax.shard_map(step, mesh=fine, in_specs=in_specs, out_specs=out_specs, check_vma=False)
```

```python
import jax
import jax.numpy as jnp
from jax import lax
from jax.experimental import pallas as pl
from jax.experimental.pallas import tpu as pltpu
from jax.sharding import Mesh
from jax.sharding import PartitionSpec as P


norm_eps = 1e-06
bf16 = jnp.bfloat16
f32 = jnp.float32

AXES = ("gr", "zl", "yh", "yl", "x", "core")
SIZES = (2, 4, 4, 2, 4, 2)
FS = ("zl", "yh", "yl")
GT = ("gr", "x", "core")
SWAP = [(0, 1), (1, 0)]


def device(gr, fs, tp):
    return gr * 256 + fs * 8 + tp


def everyone():
    return [(gr, fs, tp) for gr in range(2) for fs in range(32) for tp in range(8)]


def weight_moves():
    moves = []
    for gr, fs, tp in everyone():
        to = device(fs >> 4, 2 * (8 * gr + tp) + (fs & 1), (fs >> 1) & 7)
        moves.append((device(gr, fs, tp), to))
    return moves


def in_vmem(value):
    return pltpu.with_memory_space_constraint(value, pltpu.VMEM)


def kernel(body, outs, scratch=()):
    here = pl.BlockSpec(memory_space=pltpu.VMEM)

    def call(*args):
        return pl.pallas_call(
            body,
            in_specs=[here] * len(args),
            out_specs=tuple(here for _ in outs),
            out_shape=tuple(pltpu.VMEM(shape, bf16) for shape in outs),
            scratch_shapes=[pltpu.VMEM(shape, bf16) for shape in scratch],
            compiler_params=pltpu.CompilerParams(vmem_limit_bytes=24 << 20),
        )(*[in_vmem(a) for a in args])

    return call


def in_order(first, second, swapped):
    return jnp.where(swapped, second, first), jnp.where(swapped, first, second)


def to_everyone(value, axes, count):
    return lax.all_to_all(
        jnp.broadcast_to(value[None], (count, *value.shape)), axes, 0, 0, tiled=True
    )


def layer_call(late, normed, own, other, outputs):
    layer = 1 if late else 0

    def body(normed, own, other, *refs):
        gates, ups, serveds, part, wide, down, gate, up, served, done, *more = refs[3 * layer :]
        if late:
            fetch = pltpu.make_async_copy(other, more[0], done.at[3])
            fetch.start()
        core = lax.axis_index("core")
        even = lax.axis_index("yl") == 0

        def place(blocks, c):
            for k in range(4):
                x = lax.axis_index("x") ^ k if late else k
                for b in range(2):
                    for s in range(2):
                        line = blocks[k, b, 128 * s : 128 * s + 128]
                        wide[s, x, c, 64 * b : 64 * b + 64, :256] = line[:64]
                        wide[s, x, c, 64 * b : 64 * b + 64, 256:] = line[64:]
                    line = blocks[k, b, 256:384]
                    for g in range(2):
                        columns = line[:, 128 * g : 128 * g + 128]
                        down[g, x, c, 128 * b : 128 * b + 128] = columns

        place(own, core)
        if late:
            fetch.wait()
        place(more[0] if late else other, 1 - core)
        act = jnp.zeros((128, 512), f32)
        for s in range(2):
            for x in range(4):
                at = 1024 * s + 256 * x
                block = wide[s, x].reshape(256, 512)
                gate[at : at + 256] = jnp.where(even, block[:, :128], block[:, 128:256])
                up[at : at + 256] = jnp.where(even, block[:, 256:384], block[:, 384:])
        for g in range(2):
            for x in range(4):
                for c in range(2):
                    at = 1024 * g + 256 * x + 128 * c
                    block = down[g, x, c]
                    served[:, at : at + 128] = jnp.where(even, block[:128], block[128:])
        copies = [
            pltpu.make_async_copy(a, b.at[layer], done.at[i])
            for i, (a, b) in enumerate(((gate, gates), (up, ups), (served, serveds)))
        ]
        for copy in copies:
            copy.start()
        for s in range(2):
            for x in range(4):
                at = 1024 * s + 256 * x
                block = wide[s, x].reshape(256, 512)
                act = act + jnp.dot(normed[:, at : at + 256], block, preferred_element_type=f32)
        gate_act, up_act = act[:, :256], act[:, 256:]
        hidden = (gate_act / (1.0 + jnp.exp(-gate_act)) * up_act).astype(bf16)
        for g in range(2):
            for x in range(4):
                at = 1024 * g + 256 * x
                block = jnp.concatenate([down[g, x, 0], down[g, x, 1]], axis=1)
                out = jnp.dot(hidden, block, preferred_element_type=f32)
                part[:, at : at + 256] = out.astype(bf16)
        for copy in copies:
            copy.wait()

    here = pl.BlockSpec(memory_space=pltpu.VMEM)
    there = pl.BlockSpec(memory_space=pl.ANY)
    blocks = [pltpu.VMEM(other.shape, bf16)] if late else []
    scratch = ((2, 4, 2, 128, 512), (2, 4, 2, 256, 128), (2048, 128), (2048, 128), (128, 2048))
    shapes = ((2, 2048, 128), (2, 2048, 128), (2, 128, 2048))
    return pl.pallas_call(
        body,
        in_specs=[here, here, there if late else here] + [there] * len(outputs),
        out_specs=(there, there, there, here),
        out_shape=(
            *(jax.ShapeDtypeStruct(shape, bf16) for shape in shapes),
            pltpu.VMEM((128, 2048), bf16),
        ),
        input_output_aliases={3 + i: i for i in range(len(outputs))},
        scratch_shapes=[
            *(pltpu.VMEM(shape, bf16) for shape in scratch),
            pltpu.SemaphoreType.DMA((4,)),
            *blocks,
        ],
        compiler_params=pltpu.CompilerParams(vmem_limit_bytes=24 << 20),
        name="late_layer" if late else "early_layer",
    )(in_vmem(normed), in_vmem(own), other if late else in_vmem(other), *outputs)


def normalised(value):
    mean = jnp.sum(value * value, axis=1, keepdims=True) * (1.0 / 2048)
    return (value * lax.rsqrt(mean + norm_eps)).astype(bf16)


def norm_call(stream):
    def body(stream, out):
        out[...] = normalised(stream[...].astype(f32))

    return kernel(body, (stream.shape,))(stream)[0]


def fold_call(last, parts, mine):
    count = 32 if last else 16

    def body(parts, mine, sends, total):
        value = mine[...]
        summed = parts[0].astype(f32)
        for i in range(1, 16):
            summed = summed + parts[i].astype(f32)
        value = value + 0.5 * summed
        total[...] = value
        sent = value.astype(bf16) if last else normalised(value)
        for i in range(count):
            sends[i] = sent

    here = pl.BlockSpec(memory_space=pltpu.VMEM)
    return pl.pallas_call(
        body,
        in_specs=[here, here],
        out_specs=(here, here),
        out_shape=(pltpu.VMEM((count, 8, 2048), bf16), pltpu.VMEM((8, 2048), f32)),
        compiler_params=pltpu.CompilerParams(vmem_limit_bytes=24 << 20),
        name="fold",
    )(in_vmem(parts), in_vmem(mine))


def step(prompt, norm_gain, gate_weight, up_weight, down_weight):
    gain = norm_gain[:, :, None]
    gate = (gain * gate_weight).astype(bf16)
    up = (gain * up_weight).astype(bf16)
    high = lax.axis_index("gr") == 1
    moved = []
    for layer in range(2):
        block = jnp.concatenate([gate[layer], up[layer]], axis=0)
        moved.append(lax.ppermute(block, AXES, weight_moves()))
    down = down_weight.astype(bf16)

    def with_down(layer):
        packed = jnp.concatenate([down[layer, :64], down[layer, 64:]], axis=1)
        return jnp.concatenate([moved[layer], packed], axis=0)

    def unpacked(low, top):
        upper = jnp.concatenate([low[128:, :128], top[128:, :128]], axis=1)
        lower = jnp.concatenate([low[128:, 128:], top[128:, 128:]], axis=1)
        return jnp.concatenate([low[:128], top[:128], upper, lower], axis=0)

    both = with_down(0)
    across = lax.ppermute(both, "gr", SWAP)
    block = unpacked(*in_order(both, across, high))

    own = to_everyone(block, ("x", "yl"), 8)
    both = with_down(1)
    across = lax.ppermute(both, "gr", SWAP)
    block = unpacked(*in_order(both, across, high))
    yl = lax.axis_index("yl")
    came = lax.ppermute(block, "yl", SWAP)
    own, block = lax.optimization_barrier((own, block))
    other = lax.ppermute(own, "core", SWAP)
    pair = jnp.stack(in_order(block, came, yl == 1))
    late = [lax.ppermute(pair, "x", [(x, x ^ k) for x in range(4)]) for k in (1, 2, 3)]
    late = jnp.stack([pair, *late])
    late_other = lax.ppermute(late, "core", SWAP)

    half = lax.dynamic_slice_in_dim(prompt[0], yl * 128, 128, 0)
    mine = lax.dynamic_slice_in_dim(half, lax.axis_index(("zl", "yh")) * 8, 8, 0).astype(f32)
    normed = norm_call(half)
    early = [a.reshape(4, 2, 384, 256) for a in (own, other)]
    outputs = ()
    for layer in range(2):
        pieces = (late, late_other) if layer else early
        *outputs, part = layer_call(layer == 1, normed, *pieces, outputs)
        parts = lax.all_to_all(part.reshape(16, 8, 2048), ("zl", "yh"), 0, 0, tiled=True)
        sends, mine = fold_call(layer == 1, parts, mine)
        axes = ("yl", "zl", "yh") if layer else ("zl", "yh")
        normed = lax.all_to_all(sends, axes, 0, 0, tiled=True).reshape(-1, 2048)
    return *outputs, normed.reshape(prompt.shape)


def solution(mesh):
    fine = Mesh(mesh.devices.reshape(SIZES), AXES)
    in_specs = (P(GT, None, None), P(None, FS), P(None, FS, GT), P(None, FS, GT), P(None, FS, GT))
    out_specs = (P(None, None, FS), P(None, None, FS), P(None, FS, None), P(GT, None, None))
    return jax.shard_map(step, mesh=fine, in_specs=in_specs, out_specs=out_specs, check_vma=False)
```

```python
import jax
import jax.numpy as jnp
from jax import lax
from jax.experimental import pallas as pl
from jax.experimental.pallas import tpu as pltpu
from jax.sharding import Mesh
from jax.sharding import PartitionSpec as P


norm_eps = 1e-06
bf16 = jnp.bfloat16
f32 = jnp.float32

AXES = ("gr", "zl", "yh", "yl", "x", "core")
SIZES = (2, 4, 4, 2, 4, 2)
FS = ("zl", "yh", "yl")
GT = ("gr", "x", "core")
SWAP = [(0, 1), (1, 0)]


def device(gr, fs, tp):
    return gr * 256 + fs * 8 + tp


def everyone():
    return [(gr, fs, tp) for gr in range(2) for fs in range(32) for tp in range(8)]


def weight_moves():
    moves = []
    for gr, fs, tp in everyone():
        to = device(fs >> 4, 2 * (8 * gr + tp) + (fs & 1), (fs >> 1) & 7)
        moves.append((device(gr, fs, tp), to))
    return moves


def in_vmem(value):
    return pltpu.with_memory_space_constraint(value, pltpu.VMEM)


def kernel(body, outs, scratch=()):
    here = pl.BlockSpec(memory_space=pltpu.VMEM)

    def call(*args):
        return pl.pallas_call(
            body,
            in_specs=[here] * len(args),
            out_specs=tuple(here for _ in outs),
            out_shape=tuple(pltpu.VMEM(shape, bf16) for shape in outs),
            scratch_shapes=[pltpu.VMEM(shape, bf16) for shape in scratch],
            compiler_params=pltpu.CompilerParams(vmem_limit_bytes=24 << 20),
        )(*[in_vmem(a) for a in args])

    return call


def in_order(first, second, swapped):
    return jnp.where(swapped, second, first), jnp.where(swapped, first, second)


def to_everyone(value, axes, count):
    return lax.all_to_all(
        jnp.broadcast_to(value[None], (count, *value.shape)), axes, 0, 0, tiled=True
    )


def layer_call(late, normed, own, other, outputs):
    layer = 1 if late else 0

    def body(normed, own, other, *refs):
        gates, ups, serveds, part, wide, down, gate, up, served, done = refs[3 * layer :]
        core = lax.axis_index("core") == 0
        even = lax.axis_index("yl") == 0
        for k in range(4):
            x = lax.axis_index("x") ^ k if late else k
            for b in range(2):
                for s in range(3):
                    mn = own[k, b, 128 * s : 128 * s + 128]
                    ot = other[k, b, 128 * s : 128 * s + 128]
                    for c in range(2):
                        line = jnp.where(core, mn, ot) if c == 0 else jnp.where(core, ot, mn)
                        at = 128 * c + 64 * b
                        if s < 2:
                            wide[s, x, at : at + 64, :256] = line[:64]
                            wide[s, x, at : at + 64, 256:] = line[64:]
                        else:
                            for g in range(2):
                                down[g, x, 128 * b : 128 * b + 128, 128 * c : 128 * c + 128] = line[
                                    :, 128 * g : 128 * g + 128
                                ]
        act = jnp.zeros((128, 512), f32)
        for s in range(2):
            for x in range(4):
                at = 1024 * s + 256 * x
                block = wide[s, x]
                gate[at : at + 256] = jnp.where(even, block[:, :128], block[:, 128:256])
                up[at : at + 256] = jnp.where(even, block[:, 256:384], block[:, 384:])
        copies = [
            pltpu.make_async_copy(a, b.at[layer], done.at[i])
            for i, (a, b) in enumerate(((gate, gates), (up, ups), (served, serveds)))
        ]
        for copy in copies[:2]:
            copy.start()
        for g in range(2):
            for x in range(4):
                block = down[g, x]
                at = 1024 * g + 256 * x
                served[:, at : at + 256] = jnp.where(even, block[:128], block[128:])
        copies[2].start()
        for s in range(2):
            for x in range(4):
                at = 1024 * s + 256 * x
                act = act + jnp.dot(
                    normed[:, at : at + 256], wide[s, x], preferred_element_type=f32
                )
        gate_act, up_act = act[:, :256], act[:, 256:]
        hidden = (gate_act / (1.0 + jnp.exp(-gate_act)) * up_act).astype(bf16)
        for g in range(2):
            for x in range(4):
                at = 1024 * g + 256 * x
                out = jnp.dot(hidden, down[g, x], preferred_element_type=f32)
                part[:, at : at + 256] = out.astype(bf16)
        for copy in copies:
            copy.wait()

    here = pl.BlockSpec(memory_space=pltpu.VMEM)
    there = pl.BlockSpec(memory_space=pl.ANY)
    scratch = ((2, 4, 256, 512), (2, 4, 256, 256), (2048, 128), (2048, 128), (128, 2048))
    shapes = ((2, 2048, 128), (2, 2048, 128), (2, 128, 2048))
    return pl.pallas_call(
        body,
        in_specs=[here] * 3 + [there] * len(outputs),
        out_specs=(there, there, there, here),
        out_shape=(
            *(jax.ShapeDtypeStruct(shape, bf16) for shape in shapes),
            pltpu.VMEM((128, 2048), bf16),
        ),
        input_output_aliases={3 + i: i for i in range(len(outputs))},
        scratch_shapes=[
            *(pltpu.VMEM(shape, bf16) for shape in scratch),
            pltpu.SemaphoreType.DMA((3,)),
        ],
        compiler_params=pltpu.CompilerParams(vmem_limit_bytes=24 << 20),
        name="late_layer" if late else "early_layer",
    )(in_vmem(normed), in_vmem(own), in_vmem(other), *outputs)


def normalised(value):
    mean = jnp.sum(value * value, axis=1, keepdims=True) * (1.0 / 2048)
    return (value * lax.rsqrt(mean + norm_eps)).astype(bf16)


def norm_call(stream):
    def body(stream, out):
        out[...] = normalised(stream[...].astype(f32))

    return kernel(body, (stream.shape,))(stream)[0]


def fold_call(last, parts, mine):
    count = 32 if last else 16

    def body(parts, mine, sends, total):
        value = mine[...]
        summed = parts[0].astype(f32)
        for i in range(1, 16):
            summed = summed + parts[i].astype(f32)
        value = value + 0.5 * summed
        total[...] = value
        sent = value.astype(bf16) if last else normalised(value)
        for i in range(count):
            sends[i] = sent

    here = pl.BlockSpec(memory_space=pltpu.VMEM)
    return pl.pallas_call(
        body,
        in_specs=[here, here],
        out_specs=(here, here),
        out_shape=(pltpu.VMEM((count, 8, 2048), bf16), pltpu.VMEM((8, 2048), f32)),
        compiler_params=pltpu.CompilerParams(vmem_limit_bytes=24 << 20),
        name="fold",
    )(in_vmem(parts), in_vmem(mine))


def step(prompt, norm_gain, gate_weight, up_weight, down_weight):
    gain = norm_gain[:, :, None]
    gate = [(gain[0] * gate_weight[0]).astype(bf16)]
    up = [(gain[0] * up_weight[0]).astype(bf16)]
    gate[0], up[0], later = lax.optimization_barrier((gate[0], up[0], gain[1]))
    gate.append((later * gate_weight[1]).astype(bf16))
    up.append((later * up_weight[1]).astype(bf16))
    high = lax.axis_index("gr") == 1
    moved = []
    for layer in range(2):
        block = jnp.concatenate([gate[layer], up[layer]], axis=0)
        moved.append(lax.ppermute(block, AXES, weight_moves()))
    down = down_weight.astype(bf16)

    def with_down(layer):
        packed = jnp.concatenate([down[layer, :64], down[layer, 64:]], axis=1)
        return jnp.concatenate([moved[layer], packed], axis=0)

    def unpacked(low, top):
        upper = jnp.concatenate([low[128:, :128], top[128:, :128]], axis=1)
        lower = jnp.concatenate([low[128:, 128:], top[128:, 128:]], axis=1)
        return jnp.concatenate([low[:128], top[:128], upper, lower], axis=0)

    both = with_down(0)
    across = lax.ppermute(both, "gr", SWAP)
    block = unpacked(*in_order(both, across, high))

    own = to_everyone(block, ("x", "yl"), 8)
    both = with_down(1)
    across = lax.ppermute(both, "gr", SWAP)
    block = unpacked(*in_order(both, across, high))
    yl = lax.axis_index("yl")
    came = lax.ppermute(block, "yl", SWAP)
    own, block = lax.optimization_barrier((own, block))
    other = lax.ppermute(own, "core", SWAP)
    pair = jnp.stack(in_order(block, came, yl == 1))
    late = [lax.ppermute(pair, "x", [(x, x ^ k) for x in range(4)]) for k in (1, 2, 3)]
    late = jnp.stack([pair, *late])
    late_other = lax.ppermute(late, "core", SWAP)

    half = lax.dynamic_slice_in_dim(prompt[0], yl * 128, 128, 0)
    mine = lax.dynamic_slice_in_dim(half, lax.axis_index(("zl", "yh")) * 8, 8, 0).astype(f32)
    normed = norm_call(half)
    early = [a.reshape(4, 2, 384, 256) for a in (own, other)]
    outputs = ()
    for layer in range(2):
        pieces = (late, late_other) if layer else early
        *outputs, part = layer_call(layer == 1, normed, *pieces, outputs)
        parts = lax.all_to_all(part.reshape(16, 8, 2048), ("zl", "yh"), 0, 0, tiled=True)
        sends, mine = fold_call(layer == 1, parts, mine)
        axes = ("yl", "zl", "yh") if layer else ("zl", "yh")
        normed = lax.all_to_all(sends, axes, 0, 0, tiled=True).reshape(-1, 2048)
    return *outputs, normed.reshape(prompt.shape)


def solution(mesh):
    fine = Mesh(mesh.devices.reshape(SIZES), AXES)
    in_specs = (P(GT, None, None), P(None, FS), P(None, FS, GT), P(None, FS, GT), P(None, FS, GT))
    out_specs = (P(None, None, FS), P(None, None, FS), P(None, FS, None), P(GT, None, None))
    return jax.shard_map(step, mesh=fine, in_specs=in_specs, out_specs=out_specs, check_vma=False)
```

```python
import jax
import jax.numpy as jnp
from jax import lax
from jax.experimental import pallas as pl
from jax.experimental.pallas import tpu as pltpu
from jax.sharding import Mesh
from jax.sharding import PartitionSpec as P


norm_eps = 1e-06
bf16 = jnp.bfloat16
f32 = jnp.float32

AXES = ("gr", "zl", "yh", "yl", "x", "core")
SIZES = (2, 4, 4, 2, 4, 2)
FS = ("zl", "yh", "yl")
GT = ("gr", "x", "core")
SWAP = [(0, 1), (1, 0)]


def device(gr, fs, tp):
    return gr * 256 + fs * 8 + tp


def everyone():
    return [(gr, fs, tp) for gr in range(2) for fs in range(32) for tp in range(8)]


def weight_moves():
    moves = []
    for gr, fs, tp in everyone():
        to = device(fs >> 4, 2 * (8 * gr + tp) + (fs & 1), (fs >> 1) & 7)
        moves.append((device(gr, fs, tp), to))
    return moves


def in_vmem(value):
    return pltpu.with_memory_space_constraint(value, pltpu.VMEM)


def kernel(body, outs, scratch=()):
    here = pl.BlockSpec(memory_space=pltpu.VMEM)

    def call(*args):
        return pl.pallas_call(
            body,
            in_specs=[here] * len(args),
            out_specs=tuple(here for _ in outs),
            out_shape=tuple(pltpu.VMEM(shape, bf16) for shape in outs),
            scratch_shapes=[pltpu.VMEM(shape, bf16) for shape in scratch],
            compiler_params=pltpu.CompilerParams(vmem_limit_bytes=24 << 20),
        )(*[in_vmem(a) for a in args])

    return call


def in_order(first, second, swapped):
    return jnp.where(swapped, second, first), jnp.where(swapped, first, second)


def to_everyone(value, axes, count):
    return lax.all_to_all(
        jnp.broadcast_to(value[None], (count, *value.shape)), axes, 0, 0, tiled=True
    )


def layer_call(late, normed, own, other, outputs):
    layer = 1 if late else 0

    def body(normed, own, other, *refs):
        gates, ups, serveds, part, wide, down, gate, up, served, done = refs[3 * layer :]
        core = lax.axis_index("core") == 0
        even = lax.axis_index("yl") == 0
        for k in range(4):
            x = lax.axis_index("x") ^ k if late else k
            for b in range(2):
                for s in range(3):
                    mn = own[k, b, 128 * s : 128 * s + 128]
                    ot = other[k, b, 128 * s : 128 * s + 128]
                    for c in range(2):
                        line = jnp.where(core, mn, ot) if c == 0 else jnp.where(core, ot, mn)
                        at = 128 * c + 64 * b
                        if s < 2:
                            wide[s, x, at : at + 64, :256] = line[:64]
                            wide[s, x, at : at + 64, 256:] = line[64:]
                        else:
                            for g in range(2):
                                down[g, x, 128 * b : 128 * b + 128, 128 * c : 128 * c + 128] = line[
                                    :, 128 * g : 128 * g + 128
                                ]
        act = jnp.zeros((128, 512), f32)
        for s in range(2):
            for x in range(4):
                at = 1024 * s + 256 * x
                block = wide[s, x]
                gate[at : at + 256] = jnp.where(even, block[:, :128], block[:, 128:256])
                up[at : at + 256] = jnp.where(even, block[:, 256:384], block[:, 384:])
        for g in range(2):
            for x in range(4):
                block = down[g, x]
                at = 1024 * g + 256 * x
                served[:, at : at + 256] = jnp.where(even, block[:128], block[128:])
        copies = [
            pltpu.make_async_copy(a, b.at[layer], done.at[i])
            for i, (a, b) in enumerate(((gate, gates), (up, ups), (served, serveds)))
        ]
        for copy in copies:
            copy.start()
        for s in range(2):
            for x in range(4):
                at = 1024 * s + 256 * x
                act = act + jnp.dot(
                    normed[:, at : at + 256], wide[s, x], preferred_element_type=f32
                )
        gate_act, up_act = act[:, :256], act[:, 256:]
        hidden = (gate_act / (1.0 + jnp.exp(-gate_act)) * up_act).astype(bf16)
        for g in range(2):
            for x in range(4):
                at = 1024 * g + 256 * x
                out = jnp.dot(hidden, down[g, x], preferred_element_type=f32)
                part[:, at : at + 256] = out.astype(bf16)
        for copy in copies:
            copy.wait()

    here = pl.BlockSpec(memory_space=pltpu.VMEM)
    there = pl.BlockSpec(memory_space=pl.ANY)
    scratch = ((2, 4, 256, 512), (2, 4, 256, 256), (2048, 128), (2048, 128), (128, 2048))
    shapes = ((2, 2048, 128), (2, 2048, 128), (2, 128, 2048))
    return pl.pallas_call(
        body,
        in_specs=[here] * 3 + [there] * len(outputs),
        out_specs=(there, there, there, here),
        out_shape=(
            *(jax.ShapeDtypeStruct(shape, bf16) for shape in shapes),
            pltpu.VMEM((128, 2048), bf16),
        ),
        input_output_aliases={3 + i: i for i in range(len(outputs))},
        scratch_shapes=[
            *(pltpu.VMEM(shape, bf16) for shape in scratch),
            pltpu.SemaphoreType.DMA((3,)),
        ],
        compiler_params=pltpu.CompilerParams(vmem_limit_bytes=24 << 20),
        name="late_layer" if late else "early_layer",
    )(in_vmem(normed), in_vmem(own), in_vmem(other), *outputs)


def normalised(value):
    mean = jnp.sum(value * value, axis=1, keepdims=True) * (1.0 / 2048)
    return (value * lax.rsqrt(mean + norm_eps)).astype(bf16)


def norm_call(stream):
    def body(stream, out):
        out[...] = normalised(stream[...].astype(f32))

    return kernel(body, (stream.shape,))(stream)[0]


def fold_call(last, parts, mine):
    count = 32 if last else 16

    def body(parts, mine, sends, total):
        value = mine[...]
        summed = parts[0].astype(f32)
        for i in range(1, 16):
            summed = summed + parts[i].astype(f32)
        value = value + 0.5 * summed
        total[...] = value
        sent = value.astype(bf16) if last else normalised(value)
        for i in range(count):
            sends[i] = sent

    here = pl.BlockSpec(memory_space=pltpu.VMEM)
    return pl.pallas_call(
        body,
        in_specs=[here, here],
        out_specs=(here, here),
        out_shape=(pltpu.VMEM((count, 8, 2048), bf16), pltpu.VMEM((8, 2048), f32)),
        compiler_params=pltpu.CompilerParams(vmem_limit_bytes=24 << 20),
        name="fold",
    )(in_vmem(parts), in_vmem(mine))


def step(prompt, norm_gain, gate_weight, up_weight, down_weight):
    gain = norm_gain[:, :, None]
    gate = (gain * gate_weight).astype(bf16)
    up = (gain * up_weight).astype(bf16)
    high = lax.axis_index("gr") == 1
    moved = []
    for layer in range(2):
        block = jnp.concatenate([gate[layer], up[layer]], axis=0)
        moved.append(lax.ppermute(block, AXES, weight_moves()))
    down = down_weight.astype(bf16)

    def with_down(layer):
        packed = jnp.concatenate([down[layer, :64], down[layer, 64:]], axis=1)
        return jnp.concatenate([moved[layer], packed], axis=0)

    def unpacked(low, top):
        upper = jnp.concatenate([low[128:, :128], top[128:, :128]], axis=1)
        lower = jnp.concatenate([low[128:, 128:], top[128:, 128:]], axis=1)
        return jnp.concatenate([low[:128], top[:128], upper, lower], axis=0)

    both = with_down(0)
    across = lax.ppermute(both, "gr", SWAP)
    block = unpacked(*in_order(both, across, high))

    own = to_everyone(block, ("x", "yl"), 8)
    both = with_down(1)
    across = lax.ppermute(both, "gr", SWAP)
    block = unpacked(*in_order(both, across, high))
    yl = lax.axis_index("yl")
    came = lax.ppermute(block, "yl", SWAP)
    own, block = lax.optimization_barrier((own, block))
    other = lax.ppermute(own, "core", SWAP)
    pair = jnp.stack(in_order(block, came, yl == 1))
    late = [lax.ppermute(pair, "x", [(x, x ^ k) for x in range(4)]) for k in (1, 2, 3)]
    late = jnp.stack([pair, *late])
    late_other = lax.ppermute(late, "core", SWAP)

    half = lax.dynamic_slice_in_dim(prompt[0], yl * 128, 128, 0)
    mine = lax.dynamic_slice_in_dim(half, lax.axis_index(("yh", "zl")) * 8, 8, 0).astype(f32)
    normed = norm_call(half)
    early = [a.reshape(4, 2, 384, 256) for a in (own, other)]
    outputs = ()
    for layer in range(2):
        pieces = (late, late_other) if layer else early
        *outputs, part = layer_call(layer == 1, normed, *pieces, outputs)
        parts = lax.all_to_all(part.reshape(16, 8, 2048), ("yh", "zl"), 0, 0, tiled=True)
        sends, mine = fold_call(layer == 1, parts, mine)
        axes = ("yl", "yh", "zl") if layer else ("yh", "zl")
        normed = lax.all_to_all(sends, axes, 0, 0, tiled=True).reshape(-1, 2048)
    return *outputs, normed.reshape(prompt.shape)


def solution(mesh):
    fine = Mesh(mesh.devices.reshape(SIZES), AXES)
    in_specs = (P(GT, None, None), P(None, FS), P(None, FS, GT), P(None, FS, GT), P(None, FS, GT))
    out_specs = (P(None, None, FS), P(None, None, FS), P(None, FS, None), P(GT, None, None))
    return jax.shard_map(step, mesh=fine, in_specs=in_specs, out_specs=out_specs, check_vma=False)
```
